256 devices in a mesh: grp: 2 (over y), tp: 16 (over z), dp: 8 (over x, core).
Axes of the slice: x: 4, y: 2, z: 16, core: 2. Of those that a mesh axis runs over, the one named last changes fastest.
The devices are a block of a 4x16x16 slice.
Arguments:
- tokens: bfloat16 [128, 8, 4096], P(('grp', 'tp'), None, 'dp'), parts along dimension 0, may hold values from -6 to 6
- lengths: int32 [128], P('grp'), parts along dimension 0, may hold values from 1 to 8, 224 in all
- norm_gain: float32 [2, 4096], P(None, 'dp'), may hold values from 0.1 to 1.9
- w_recept: bfloat16 [2, 4096, 2048], P(None, 'dp', 'tp'), may hold values from -0.09375 to 0.09375
- w_key: bfloat16 [2, 4096, 2048], P(None, 'dp', 'tp'), may hold values from -0.09375 to 0.09375
- w_value: bfloat16 [2, 4096, 2048], P(None, 'dp', 'tp'), may hold values from -0.09375 to 0.09375
- w_decay: bfloat16 [2, 4096, 2048], P(None, 'dp', 'tp'), may hold values from -0.375 to 0.375
- w_rate: bfloat16 [2, 4096, 2048], P(None, 'dp', 'tp'), may hold values from -0.09375 to 0.09375
- w_gate: bfloat16 [2, 4096, 2048], P(None, 'dp', 'tp'), may hold values from -0.09375 to 0.09375
- w_out: bfloat16 [2, 2048, 4096], P(None, 'tp', 'dp'), may hold values from -0.125 to 0.125
- decay_base: float32 [2, 2048], P(None, 'tp'), may hold values from -4 to 3
- out_gain: float32 [2, 2048], P(None, 'tp'), may hold values from 0.1 to 1.9
- states: float32 [2, 128, 64, 2048], P(None, ('grp', 'dp'), None, 'tp'), parts along dimension 1, may hold values from -6 to 6
Outputs:
- stream_out: float32 [128, 8, 4096], P(('grp', 'tp'), None, 'dp'), parts along dimension 0
- new_states: float32 [2, 128, 64, 2048], P(None, ('grp', 'dp'), None, 'tp'), parts along dimension 1
The draws below stay inside these ranges and needn't reach their ends.
There are 2 independent parts, one for each index of `grp`. The reference program is written for one: setup_inputs(seed, part) draws one part's arguments, and reference() takes and returns one part's arrays. A program takes and returns all parts, laid end to end along the dimension named above; an argument that names none is the same for every part. Nothing has to cross between parts.
Inputs may be any that keep to these rules, and one draw needn't show every extreme that they name: lengths[b] first tokens of sequence b are live; together they count 7 * 32 and the largest is 8.
All inputs are finite; a program needn't handle non-finite values.
Results may differ from the reference program's by a relative error of at most 0.0061.
Values may be sent and summed in bfloat16 or wider, within the bound.
No kernel may reach another device: no remote copies, remote signals or barrier semaphores. Data moves between devices by JAX's collectives and lax.ppermute only.
A program may use at most 128 MiB of HBM per device.

```python
import math
import jax
import jax.numpy as jnp
import numpy as np
from jax import lax

D = 4096
HEAD = 64
WIDTH = 2048
STEPS = 8
BLOCKS = 2
SEQS = 64


def draw_tokens(key, part):
    row_key, column_key, value_key = jax.random.split(key, 3)
    rising = jnp.exp(jnp.linspace(math.log(0.5), math.log(2.0), D))
    rough = jax.random.uniform(column_key, (D,), jnp.float32, 0.6, 1.5)
    row_scale = jnp.exp(jax.random.uniform(row_key, (SEQS, STEPS, 1), jnp.float32, math.log(0.1), math.log(1.0)))
    values = jax.random.normal(value_key, (SEQS, STEPS, D), jnp.float32)
    drawn = jnp.clip(values * row_scale * rising * rough, -6.0, 6.0)
    return drawn.astype(jnp.bfloat16)


def steps_of(key, shape, shards, least, high):
    def one(dim, parts):
        heights = jax.random.uniform(jax.random.fold_in(jax.random.fold_in(key, 6), dim), (parts,), jnp.float32, least / len(shards), high / len(shards))
        return jnp.repeat(jnp.exp(heights), shape[dim] // parts).reshape((-1,) + (1,) * (len(shape) - dim - 1))

    level = one(*shards[0])
    for cut in shards[1:]:
        level = level * one(*cut)
    return level


def length_profile(count, total, bound, skew):
    weights = [(1 << 20) // math.isqrt(grade ** skew) + 1 for grade in range(2, count + 1)]
    surplus, given = total - bound - (count - 1), [1] * (count - 1)
    while surplus > 0:
        movable = [i for i in range(count - 1) if given[i] < bound]
        whole, budget = sum([weights[i] for i in movable]), surplus
        for i in movable:
            extra = min(bound - given[i], max(1, budget * weights[i] // whole), surplus)
            given[i] = given[i] + extra
            surplus = surplus - extra
    return np.array([bound] + given)


def ragged_sizes(stream_key, number_of, total, most, skew):
    if number_of == 2:
        one = jax.random.randint(stream_key, (), max(1, total - most), min(most, total - 1) + 1)
        return jnp.stack([one, total - one])
    tallies = jnp.asarray(length_profile(number_of, total, most, skew), jnp.int32)
    twos = (number_of - 1) // 2
    donor, taker = tallies[1:1 + 2 * twos:2], tallies[2:2 + 2 * twos:2]
    margin = jnp.minimum(donor - 1, most - taker)
    moved = jax.random.randint(jax.random.fold_in(stream_key, 1), (twos,), 0, 1 << 20) % (margin + 1)
    tallies = tallies.at[1:1 + 2 * twos:2].set(donor - moved).at[2:2 + 2 * twos:2].set(taker + moved)
    return tallies[jax.random.permutation(jax.random.fold_in(stream_key, 2), number_of)]


def bell_draw(own_key, shape, deviation, reach, pieces=(), kind=jnp.bfloat16):
    gain = steps_of(own_key, shape, pieces, -0.22, 0.18) if pieces else 1.0
    array = jax.random.normal(own_key, shape, jnp.float32) * deviation * gain
    return jnp.minimum(jnp.maximum(array, -reach), reach).astype(kind)


def setup_inputs(seed: int = 0, part: int = 0) -> dict:
    arg_keys = jax.random.split(jax.random.key(seed), 14)
    part_splits = jax.random.split(jax.random.fold_in(arg_keys[13], part), 14)
    tokens = draw_tokens(jax.random.fold_in(jax.random.fold_in(arg_keys[13], part), 71), part)
    lengths = ragged_sizes(part_splits[1], SEQS, 7 * SEQS // 2, STEPS, 2).astype(jnp.int32)
    norm_gain = jnp.clip(1.0 + 0.18 * jax.random.normal(arg_keys[2], (BLOCKS, D), jnp.float32), 0.1, 1.9)
    w_recept = bell_draw(arg_keys[3], (BLOCKS, D, WIDTH), D ** -0.5, 0.09375, ((1, 8), (2, 16)))
    w_key = bell_draw(arg_keys[4], (BLOCKS, D, WIDTH), D ** -0.5, 0.09375, ((1, 8), (2, 16)))
    w_value = bell_draw(arg_keys[5], (BLOCKS, D, WIDTH), D ** -0.5, 0.09375, ((1, 8), (2, 16)))
    w_decay = bell_draw(arg_keys[6], (BLOCKS, D, WIDTH), (D // 16) ** -0.5, 0.375, ((1, 8), (2, 16)))
    w_rate = bell_draw(arg_keys[7], (BLOCKS, D, WIDTH), D ** -0.5, 0.09375, ((1, 8), (2, 16)))
    w_gate = bell_draw(arg_keys[8], (BLOCKS, D, WIDTH), D ** -0.5, 0.09375, ((1, 8), (2, 16)))
    w_out = bell_draw(arg_keys[9], (BLOCKS, WIDTH, D), WIDTH ** -0.5, 0.125, ((1, 16), (2, 8)))
    decay_base = jnp.clip(-4.0 + 7.0 * jax.random.uniform(arg_keys[10], (BLOCKS, WIDTH), jnp.float32) ** steps_of(arg_keys[10], (BLOCKS, WIDTH), ((1, 16),), -0.2, 0.2), -4.0, 3.0)
    out_gain = jnp.clip(1.0 + 0.18 * jax.random.normal(arg_keys[11], (BLOCKS, WIDTH), jnp.float32), 0.1, 1.9)
    states = bell_draw(part_splits[12], (BLOCKS, SEQS, HEAD, WIDTH), 1.0, 6.0, ((1, 8), (3, 16)), jnp.float32)
    return {"tokens": tokens, "lengths": lengths, "norm_gain": norm_gain, "w_recept": w_recept, "w_key": w_key, "w_value": w_value, "w_decay": w_decay, "w_rate": w_rate, "w_gate": w_gate, "w_out": w_out, "decay_base": decay_base, "out_gain": out_gain, "states": states}


group_eps = 0.00064
norm_eps = 1e-06
key_eps = 1e-06
decay_scale = 0.606531
highest = lax.Precision.HIGHEST

def mix_heads(state_in, recept, keys_in, values, decay_pre, rate_pre, gate_pre, base_shift, out_scale, live_mask, head_size):
    row_count, step_count, width_all = recept.shape
    head_count = width_all // head_size
    shape_heads = (row_count, step_count, head_count, head_size)
    decay_rate = jnp.exp(-decay_scale * jax.nn.sigmoid(decay_pre + base_shift)).reshape(shape_heads)
    learn_rate = jax.nn.sigmoid(rate_pre).reshape(shape_heads)
    key_heads = keys_in.reshape(shape_heads)
    unit_keys = key_heads * lax.rsqrt(lax.optimization_barrier(jnp.sum(key_heads * key_heads, axis=3, keepdims=True)) + key_eps)
    removal = unit_keys * learn_rate
    recept_heads = recept.reshape(shape_heads)
    value_heads = values.reshape(shape_heads)
    memory = state_in.reshape(row_count, head_size, head_count, head_size)
    outputs = []
    for position in range(step_count):
        seen_part = jnp.einsum('bihj,bhj->bhi', memory, unit_keys[:, position], precision=highest)
        updated = memory * decay_rate[:, position][:, None, :, :] - jnp.swapaxes(seen_part, 1, 2)[:, :, :, None] * removal[:, position][:, None, :, :] + jnp.swapaxes(value_heads[:, position], 1, 2)[:, :, :, None] * key_heads[:, position][:, None, :, :]
        memory = jnp.where(live_mask[:, position][:, None, None, None], updated, memory)
        outputs.append(jnp.einsum('bihj,bhj->bhi', memory, recept_heads[:, position], precision=highest))
    readout = jnp.stack(outputs, axis=1)
    centered = readout - lax.optimization_barrier(jnp.mean(readout, axis=3, keepdims=True))
    normed = centered * lax.rsqrt(lax.optimization_barrier(jnp.mean(centered * centered, axis=3, keepdims=True)) + group_eps)
    gated = normed.reshape(row_count, step_count, width_all) * out_scale * jax.nn.sigmoid(gate_pre)
    gated = jnp.where(live_mask[:, :, None], gated, 0.0)
    return (gated.astype(jnp.bfloat16), memory.reshape(row_count, head_size, width_all))

def reference(tokens, lengths, norm_gain, w_recept, w_key, w_value, w_decay, w_rate, w_gate, w_out, decay_base, out_gain, states):
    live_mask = jnp.arange(STEPS, dtype=jnp.int32)[None, :] < lengths[:, None]
    current = tokens.astype(jnp.float32)
    finals = []
    for block_index in range(BLOCKS):
        inv_rms = lax.rsqrt(lax.optimization_barrier(jnp.sum(current * current, axis=2)) / D + norm_eps)
        scaled = (current * norm_gain[block_index]).astype(jnp.bfloat16).reshape(SEQS * STEPS, D)
        projected = [jnp.dot(scaled, weight[block_index], preferred_element_type=jnp.float32).reshape(SEQS, STEPS, WIDTH) * inv_rms[:, :, None] for weight in (w_recept, w_key, w_value, w_decay, w_rate, w_gate)]
        gated, final_state = mix_heads(states[block_index], projected[0], projected[1], projected[2], projected[3], projected[4], projected[5], decay_base[block_index], out_gain[block_index], live_mask, HEAD)
        finals.append(final_state)
        output = jnp.dot(gated.reshape(SEQS * STEPS, WIDTH), w_out[block_index], preferred_element_type=jnp.float32).reshape(SEQS, STEPS, D)
        current = current + output
    return (current, jnp.stack(finals, axis=0))
```

```python
import functools

import jax
import jax.numpy as jnp
from jax import lax
from jax.experimental import pallas as pl
from jax.experimental.pallas import tpu as pltpu
from jax.sharding import Mesh
from jax.sharding import PartitionSpec as P

D = 4096
HEAD = 64
BLOCKS = 2
LANES = 128
CORES = 2
LIVE = 224
SLOTS = 16
DP = ("x", "c")
GRP_DP = ("grp", "x", "c")

group_eps = 0.00064
norm_eps = 1e-06
key_eps = 1e-06
decay_scale = 0.606531

f32 = jnp.float32
bf16 = jnp.bfloat16


def iota(shape, dim):
    return lax.broadcasted_iota(jnp.int32, shape, dim)


def vmem():
    return pl.BlockSpec(memory_space=pltpu.VMEM)


def smem():
    return pl.BlockSpec(memory_space=pltpu.SMEM)


def call(kernel, out_shape, in_specs, out_specs=None, scratch=(), **more):
    if out_specs is None:
        out_specs = jax.tree.map(lambda _: vmem(), out_shape)
    return pl.pallas_call(
        kernel,
        grid=(1,),
        out_shape=out_shape,
        in_specs=in_specs,
        out_specs=out_specs,
        scratch_shapes=list(scratch),
        **more,
    )


def split_two(value):
    high = value.astype(bf16)
    low = (value - high.astype(f32)).astype(bf16)
    return jnp.concatenate([high, low], axis=1)


def head_mask():
    rows, cols = iota((2 * LANES, LANES), 0), iota((2 * LANES, LANES), 1)
    return jnp.where((rows % LANES) // HEAD == cols // HEAD, 1.0, 0.0).astype(bf16)


def head_sum(value, mask):
    return jnp.dot(split_two(value), mask, preferred_element_type=f32)


def compact_rows(lens, slots, rows, steps, first):
    seqs = rows // steps
    seq_of = iota((seqs, rows), 1) // steps
    before = jnp.where(iota((seqs, rows), 0) < seq_of, 1.0, 0.0).astype(bf16)
    same = jnp.where(iota((seqs, rows), 0) == seq_of, 1.0, 0.0).astype(bf16)
    wide = jnp.broadcast_to(lens.astype(f32), (8, seqs)).astype(bf16)
    start = jnp.dot(wide, before, preferred_element_type=f32)[0:1]
    count = jnp.dot(wide, same, preferred_element_type=f32)[0:1]
    step = (iota((1, rows), 1) % steps).astype(f32)
    place = jnp.where(step < count, start + step, -1.0)
    slot = (iota((slots, rows), 0) + first).astype(f32)
    return jnp.where(slot == jnp.broadcast_to(place, (slots, rows)), 1.0, 0.0).astype(bf16)


def spread_rows(lens, rows, slots, steps):
    seqs = rows // steps
    wide = jnp.broadcast_to(lens.astype(f32), (rows, seqs))
    seq_of = iota((rows, seqs), 0) // steps
    start = jnp.sum(jnp.where(iota((rows, seqs), 1) < seq_of, wide, 0.0), axis=1, keepdims=True)
    count = jnp.sum(jnp.where(iota((rows, seqs), 1) == seq_of, wide, 0.0), axis=1, keepdims=True)
    step = (iota((rows, 1), 0) % steps).astype(f32)
    live = step < count
    place = jnp.where(live, start + step, -1.0)
    slot = iota((rows, slots), 1).astype(f32)
    return jnp.where(slot == jnp.broadcast_to(place, (rows, slots)), 1.0, 0.0).astype(bf16), live


def two_lanes(total):
    high = total.astype(bf16).astype(f32)
    return jnp.where(iota(total.shape, 1) < LANES // 2, high, total - high)


def project(index_ref, scaled, squares, weights, keep_ref, send_ref, scaled_scr, square_scr):
    owners = scaled_scr.shape[0]
    held = scaled_scr.shape[1]
    scaled_scr[...] = scaled.reshape(scaled_scr.shape)
    square_scr[...] = jnp.broadcast_to(squares, (owners * held, LANES)).reshape(square_scr.shape)
    weight = jnp.concatenate([w[0] for w in weights], axis=1)
    width = weight.shape[1]
    core = index_ref[0]
    for target, who in ((send_ref, 1 - core), (keep_ref, core)):
        left = jnp.concatenate([scaled_scr[CORES * x + who] for x in range(owners // CORES)], axis=0)
        part = jnp.dot(left, weight, preferred_element_type=f32)
        for x in range(owners // CORES):
            target[x, :, :width] = part[x * held : (x + 1) * held].astype(target.dtype)
            square = square_scr[CORES * x + who]
            if target is send_ref:
                square = two_lanes(square)
            else:
                square = jnp.where(iota(square.shape, 1) < LANES // 2, square, 0.0)
            target[x, :, width:] = square.astype(target.dtype)


def first_kernel(index_ref, tokens_ref, gain_ref, *refs):
    weights, (keep_ref, send_ref, scaled_scr, square_scr) = refs[:6], refs[6:]
    x = tokens_ref[...].astype(f32)
    scaled = (x * gain_ref[0:1]).astype(bf16)
    squares = jnp.sum(x * x, axis=1, keepdims=True)
    project(index_ref, scaled, squares, weights, keep_ref, send_ref, scaled_scr, square_scr)


def next_kernel(steps, index_ref, lens_ref, gathered_ref, tokens_ref, gain_ref, *refs):
    weights, (keep_ref, send_ref, resid_ref, scaled_scr, square_scr, wide_scr) = refs[:6], refs[6:]
    rows = scaled_scr.shape[0] * scaled_scr.shape[1]
    spread, live = spread_rows(lens_ref[...], rows, gathered_ref.shape[0], steps)
    wide = jnp.dot(spread, gathered_ref[...], preferred_element_type=f32)
    scaled = wide.astype(bf16)
    x = wide * (1.0 / gain_ref[1:2])
    squares = jnp.sum(x * x, axis=1, keepdims=True)
    own = resid_ref.shape[0]
    wide_scr[...] = jnp.where(live, x, 0.0).reshape(wide_scr.shape)
    live_own = jnp.where(live, 1.0, 0.0)
    square_scr[...] = jnp.broadcast_to(live_own, (rows, LANES)).reshape(square_scr.shape)
    rank = index_ref[1]
    chosen = wide_scr[rank]
    per = square_scr.shape[1] // own
    alive = square_scr[rank // per, pl.ds(pl.multiple_of((rank % per) * own, own), own), 0:1] > 0.5
    resid_ref[...] = jnp.where(alive, chosen, tokens_ref[...].astype(f32))
    project(index_ref, scaled, squares, weights, keep_ref, send_ref, scaled_scr, square_scr)


def add_kernel(keep_ref, got_ref, out_ref):
    width = out_ref.shape[2] - LANES
    total = keep_ref[...] + got_ref[...].astype(f32)
    out_ref[:, :, :width] = total[:, :, :width].astype(bf16)
    for x in range(out_ref.shape[0]):
        square = total[x, :, width:]
        square = square + pltpu.roll(square, LANES // 2, 1)
        out_ref[x, :, width:] = two_lanes(square).astype(bf16)


def mix_kernel(steps, index_ref, lens_ref, parts_ref, base_ref, gain_ref, state_ref, *refs):
    gated_ref, new_ref, rows_scr, seen_scr, value_scr, read_scr = refs[-6:]
    seqs = state_ref.shape[1]
    mask = head_mask()
    total = parts_ref[0].astype(f32)
    for x in range(1, parts_ref.shape[0]):
        total = total + parts_ref[x].astype(f32)
    square = total[:, 6 * LANES :]
    square = square + pltpu.roll(square, LANES // 2, 1)
    inv_rms = lax.rsqrt(square * (1.0 / D) + norm_eps)
    recept, keys, values, decay_pre, rate_pre, gate_pre = (
        total[:, i * LANES : (i + 1) * LANES] * inv_rms for i in range(6)
    )
    first = index_ref[2] * seqs
    live = jnp.concatenate(
        [iota((steps, LANES), 0) < lens_ref[first + b] for b in range(seqs)], axis=0
    )
    decay = jnp.exp(-decay_scale * jax.nn.sigmoid(decay_pre + base_ref[...]))
    rate = jax.nn.sigmoid(rate_pre)
    unit = keys * lax.rsqrt(head_sum(keys * keys, mask) + key_eps)
    rows_scr[0] = unit
    rows_scr[1] = jnp.where(live, decay, 1.0)
    rows_scr[2] = jnp.where(live, unit * rate, 0.0)
    rows_scr[3] = jnp.where(live, keys, 0.0)
    rows_scr[4] = values
    rows_scr[5] = recept
    diagonal = iota((HEAD, LANES), 0) == iota((HEAD, LANES), 1) % HEAD

    def row(which, b, s):
        return rows_scr[which, pl.ds(b * steps + s, 1), :]

    def widened(s):
        return [jnp.where(diagonal, row(4, b, s), 0.0) for b in range(seqs)]

    left = [state_ref[0, b] * row(0, b, 0) for b in range(seqs)] + widened(0)
    sums = head_sum(jnp.concatenate(left, axis=0), mask)
    span = seqs * HEAD
    seen_scr[...] = sums[:span].reshape(seen_scr.shape)
    value_scr[...] = sums[span:].reshape(value_scr.shape)
    new_ref[0] = state_ref[0]

    def step(s, carry):
        later = jnp.minimum(s + 1, steps - 1)
        ahead, now = [], []
        for b in range(seqs):
            state = (
                new_ref[0, b] * row(1, b, s)
                - seen_scr[b] * row(2, b, s)
                + value_scr[b] * row(3, b, s)
            )
            new_ref[0, b] = state
            ahead.append(state * row(0, b, later))
            now.append(state * row(5, b, s))
        sums = head_sum(jnp.concatenate(now + ahead + widened(later), axis=0), mask)
        for b in range(seqs):
            read = jnp.where(diagonal, sums[b * HEAD : (b + 1) * HEAD], 0.0)
            read_scr[pl.ds(b * steps + s, 1), :] = jnp.sum(read, axis=0, keepdims=True)
        seen_scr[...] = sums[span : 2 * span].reshape(seen_scr.shape)
        value_scr[...] = sums[2 * span :].reshape(value_scr.shape)
        return carry

    lax.fori_loop(0, steps, step, 0)
    read = read_scr[...]
    centered = read - head_sum(read, mask) * (1.0 / HEAD)
    spread = head_sum(centered * centered, mask) * (1.0 / HEAD)
    normed = centered * lax.rsqrt(spread + group_eps)
    gated = normed * gain_ref[...] * jax.nn.sigmoid(gate_pre)
    gated = jnp.where(live, gated, 0.0).astype(bf16)
    for d in range(gated_ref.shape[0]):
        gated_ref[d] = gated


def out_compact_kernel(steps, lens_ref, gated_ref, weight_ref, out_ref):
    slots = out_ref.shape[0] * out_ref.shape[1]
    pick = compact_rows(lens_ref[...], slots, gated_ref.shape[0], steps, 0)
    rows = jnp.dot(pick, gated_ref[...], preferred_element_type=f32).astype(bf16)
    part = jnp.dot(rows, weight_ref[0], preferred_element_type=f32)
    out_ref[...] = part.astype(bf16).reshape(out_ref.shape)


def out_kernel(gated_ref, weight_ref, out_ref):
    part = jnp.dot(gated_ref[...], weight_ref[0], preferred_element_type=f32)
    out_ref[...] = part.astype(bf16).reshape(out_ref.shape)


def join_kernel(steps, index_ref, lens_ref, tokens_ref, parts_ref, gain_ref, out_ref):
    slots = parts_ref.shape[1]
    pick = compact_rows(
        lens_ref[...], slots, tokens_ref.shape[0], steps, index_ref[1] * slots
    )
    x = jnp.dot(pick, tokens_ref[...], preferred_element_type=f32)
    total = parts_ref[0].astype(f32)
    for t in range(1, parts_ref.shape[0]):
        total = total + parts_ref[t].astype(f32)
    scaled = ((x + total) * gain_ref[1:2]).astype(bf16)
    for t in range(out_ref.shape[0]):
        out_ref[t] = scaled


def final_kernel(parts_ref, resid_ref, out_ref):
    total = parts_ref[0].astype(f32)
    for t in range(1, parts_ref.shape[0]):
        total = total + parts_ref[t].astype(f32)
    out_ref[...] = resid_ref[...] + total


def body(
    tokens,
    lengths,
    norm_gain,
    w_recept,
    w_key,
    w_value,
    w_decay,
    w_rate,
    w_gate,
    w_out,
    decay_base,
    out_gain,
    states,
):
    own_seqs, steps, feats = tokens.shape
    tp, xs = lax.axis_size("tp"), lax.axis_size("x")
    owners = xs * CORES
    own = own_seqs * steps
    rows = own * tp
    held = rows // owners
    seqs = states.shape[1]
    lanes = w_key.shape[2]
    width = 6 * lanes + LANES
    assert lanes == LANES and SLOTS * tp >= LIVE and seqs * steps == held

    index = jnp.stack([lax.axis_index("c"), lax.axis_index("tp"), lax.axis_index(DP)]).astype(
        jnp.int32
    )
    lens_row = lengths.reshape(1, -1)
    mine = tokens.reshape(own, feats)
    everyone = lax.all_gather(mine, "tp", axis=0, tiled=True)
    weights = (w_recept, w_key, w_value, w_decay, w_rate, w_gate)

    def pick(block, shape):
        return pl.BlockSpec((1, *shape), lambda _: (block, *(0 for _ in shape)))

    def weight_specs(block):
        return [pick(block, (feats, lanes)) for _ in weights]

    pair = (
        jax.ShapeDtypeStruct((xs, held, width), f32),
        jax.ShapeDtypeStruct((xs, held, width), bf16),
    )
    project_scratch = (
        pltpu.VMEM((owners, held, feats), bf16),
        pltpu.VMEM((owners, held, LANES), f32),
    )

    def exchange(keep, send):
        got = lax.ppermute(send, "c", [(0, 1), (1, 0)])
        both = call(
            add_kernel, jax.ShapeDtypeStruct((xs, held, width), bf16), [vmem(), vmem()]
        )(keep, got)
        return lax.all_to_all(both, "x", 0, 0, tiled=True)

    def mixed(block, parts, news):
        out_shape = (
            jax.ShapeDtypeStruct((owners, held, lanes), bf16),
            jax.ShapeDtypeStruct(states.shape, f32),
        )
        extra = [] if news is None else [news]
        gated, news = call(
            functools.partial(mix_kernel, steps),
            out_shape,
            [smem(), smem(), vmem(), vmem(), vmem(), pick(block, states.shape[1:])]
            + [pl.BlockSpec(memory_space=pl.ANY)] * len(extra),
            (vmem(), pick(block, states.shape[1:])),
            (
                pltpu.VMEM((6, held, LANES), f32),
                pltpu.VMEM((seqs, HEAD, LANES), f32),
                pltpu.VMEM((seqs, HEAD, LANES), f32),
                pltpu.VMEM((held, LANES), f32),
            ),
            input_output_aliases={6: 1} if extra else {},
        )(
            index,
            lengths,
            parts,
            decay_base[block].reshape(1, -1),
            out_gain[block].reshape(1, -1),
            states,
            *extra,
        )
        gathered = lax.all_to_all(gated, DP, 0, 0, tiled=True)
        return gathered.reshape(rows, lanes), news

    keep, send = call(
        first_kernel,
        pair,
        [smem(), vmem(), vmem(), *weight_specs(0)],
        scratch=project_scratch,
    )(index, everyone, norm_gain, *weights)
    gated, news = mixed(0, exchange(keep, send), None)
    partial = call(
        functools.partial(out_compact_kernel, steps),
        jax.ShapeDtypeStruct((tp, SLOTS, feats), bf16),
        [vmem(), vmem(), pick(0, (lanes, feats))],
    )(lens_row, gated, w_out)
    partial = lax.all_to_all(partial, "tp", 0, 0, tiled=True)
    scaled = call(
        functools.partial(join_kernel, steps),
        jax.ShapeDtypeStruct((tp, SLOTS, feats), bf16),
        [smem(), vmem(), vmem(), vmem(), vmem()],
    )(index, lens_row, everyone, partial, norm_gain)
    scaled = lax.all_to_all(scaled, "tp", 0, 0, tiled=True).reshape(tp * SLOTS, feats)
    keep, send, resid = call(
        functools.partial(next_kernel, steps),
        (*pair, jax.ShapeDtypeStruct((own, feats), f32)),
        [smem(), vmem(), vmem(), vmem(), vmem(), *weight_specs(1)],
        scratch=(*project_scratch, pltpu.VMEM((tp, own, feats), f32)),
    )(index, lens_row, scaled, mine, norm_gain, *weights)
    gated, news = mixed(1, exchange(keep, send), news)
    partial = call(
        out_kernel,
        jax.ShapeDtypeStruct((tp, own, feats), bf16),
        [vmem(), pick(1, (lanes, feats))],
    )(gated, w_out)
    partial = lax.all_to_all(partial, "tp", 0, 0, tiled=True)
    stream = call(final_kernel, jax.ShapeDtypeStruct((own, feats), f32), [vmem(), vmem()])(
        partial, resid
    )
    return stream.reshape(tokens.shape), news


def solution(mesh):
    split = Mesh(
        mesh.devices.reshape(
            mesh.shape["grp"], mesh.shape["tp"], mesh.shape["dp"] // CORES, CORES
        ),
        ("grp", "tp", "x", "c"),
    )
    return jax.shard_map(
        body,
        mesh=split,
        in_specs=(
            P(("grp", "tp"), None, DP),
            P("grp"),
            P(None, DP),
            P(None, DP, "tp"),
            P(None, DP, "tp"),
            P(None, DP, "tp"),
            P(None, DP, "tp"),
            P(None, DP, "tp"),
            P(None, DP, "tp"),
            P(None, "tp", DP),
            P(None, "tp"),
            P(None, "tp"),
            P(None, GRP_DP, None, "tp"),
        ),
        out_specs=(P(("grp", "tp"), None, DP), P(None, GRP_DP, None, "tp")),
        check_vma=False,
    )
```

```python
import functools

import jax
import jax.numpy as jnp
from jax import lax
from jax.experimental import pallas as pl
from jax.experimental.pallas import tpu as pltpu
from jax.sharding import Mesh
from jax.sharding import PartitionSpec as P

D = 4096
HEAD = 64
BLOCKS = 2
LANES = 128
CORES = 2
LIVE = 224
SLOTS = 16
DP = ("x", "c")
GRP_DP = ("grp", "x", "c")

group_eps = 0.00064
norm_eps = 1e-06
key_eps = 1e-06
decay_scale = 0.606531


f32 = jnp.float32
bf16 = jnp.bfloat16


def iota(shape, dim):
    return lax.broadcasted_iota(jnp.int32, shape, dim)


def vmem():
    return pl.BlockSpec(memory_space=pltpu.VMEM)


def smem():
    return pl.BlockSpec(memory_space=pltpu.SMEM)


def near(value):
    return pltpu.with_memory_space_constraint(value, pltpu.VMEM)


def call(kernel, out_shape, in_specs, out_specs=None, scratch=(), **more):
    if out_specs is None:
        out_specs = tuple(vmem() for _ in out_shape) if isinstance(out_shape, tuple) else vmem()
    return pl.pallas_call(
        kernel,
        grid=(1,),
        out_shape=out_shape,
        in_specs=in_specs,
        out_specs=out_specs,
        scratch_shapes=list(scratch),
        **more,
    )


def split_two(value):
    high = value.astype(bf16)
    low = (value - high.astype(f32)).astype(bf16)
    return jnp.concatenate([high, low], axis=1)


def head_mask():
    rows, cols = iota((2 * LANES, LANES), 0), iota((2 * LANES, LANES), 1)
    return jnp.where((rows % LANES) // HEAD == cols // HEAD, 1.0, 0.0).astype(bf16)


def head_sum(value, mask):
    return jnp.dot(split_two(value), mask, preferred_element_type=f32)


def compact_rows(lens, slots, rows, steps, first):
    seqs = rows // steps
    seq_of = iota((seqs, rows), 1) // steps
    before = jnp.where(iota((seqs, rows), 0) < seq_of, 1.0, 0.0).astype(bf16)
    same = jnp.where(iota((seqs, rows), 0) == seq_of, 1.0, 0.0).astype(bf16)
    wide = jnp.broadcast_to(lens.astype(f32), (8, seqs)).astype(bf16)
    start = jnp.dot(wide, before, preferred_element_type=f32)[0:1]
    count = jnp.dot(wide, same, preferred_element_type=f32)[0:1]
    step = (iota((1, rows), 1) % steps).astype(f32)
    place = jnp.where(step < count, start + step, -1.0)
    slot = (iota((slots, rows), 0) + first).astype(f32)
    return jnp.where(slot == jnp.broadcast_to(place, (slots, rows)), 1.0, 0.0).astype(bf16)


def spread_rows(lens, rows, slots, steps):
    seqs = rows // steps
    wide = jnp.broadcast_to(lens.astype(f32), (rows, seqs))
    seq_of = iota((rows, seqs), 0) // steps
    start = jnp.sum(jnp.where(iota((rows, seqs), 1) < seq_of, wide, 0.0), axis=1, keepdims=True)
    count = jnp.sum(jnp.where(iota((rows, seqs), 1) == seq_of, wide, 0.0), axis=1, keepdims=True)
    step = (iota((rows, 1), 0) % steps).astype(f32)
    live = step < count
    place = jnp.where(live, start + step, -1.0)
    slot = iota((rows, slots), 1).astype(f32)
    return jnp.where(slot == jnp.broadcast_to(place, (rows, slots)), 1.0, 0.0).astype(bf16), live


def two_lanes(total):
    high = total.astype(bf16).astype(f32)
    return jnp.where(iota(total.shape, 1) < LANES // 2, high, total - high)


def project(scaled, squares, weights, keep_ref, send_ref, scaled_scr, square_scr):
    owners = scaled_scr.shape[0]
    held = scaled_scr.shape[1]
    scaled_scr[...] = scaled.reshape(scaled_scr.shape)
    square_scr[...] = jnp.broadcast_to(squares, (owners * held, LANES)).reshape(square_scr.shape)
    weight = jnp.concatenate([w[0] for w in weights], axis=1)
    width = weight.shape[1]
    core = lax.axis_index("c")
    for target, who in ((send_ref, 1 - core), (keep_ref, core)):
        left = jnp.concatenate([scaled_scr[CORES * x + who] for x in range(owners // CORES)], axis=0)
        part = jnp.dot(left, weight, preferred_element_type=f32)
        for x in range(owners // CORES):
            target[x, :, :width] = part[x * held : (x + 1) * held].astype(target.dtype)
            square = square_scr[CORES * x + who]
            if target is send_ref:
                square = two_lanes(square)
            else:
                square = jnp.where(iota(square.shape, 1) < LANES // 2, square, 0.0)
            target[x, :, width:] = square.astype(target.dtype)


def first_kernel(tokens_ref, gain_ref, *refs):
    weights, (keep_ref, send_ref, scaled_scr, square_scr) = refs[:6], refs[6:]
    x = tokens_ref[...].astype(f32)
    scaled = (x * gain_ref[0:1]).astype(bf16)
    squares = jnp.sum(x * x, axis=1, keepdims=True)
    project(scaled, squares, weights, keep_ref, send_ref, scaled_scr, square_scr)


def next_kernel(steps, lens_ref, gathered_ref, tokens_ref, gain_ref, *refs):
    weights, (keep_ref, send_ref, resid_ref, scaled_scr, square_scr, wide_scr) = refs[:6], refs[6:]
    rows = scaled_scr.shape[0] * scaled_scr.shape[1]
    spread, live = spread_rows(lens_ref[...], rows, gathered_ref.shape[0], steps)
    wide = jnp.dot(spread, gathered_ref[...], preferred_element_type=f32)
    scaled = wide.astype(bf16)
    x = wide * (1.0 / gain_ref[1:2])
    squares = jnp.sum(x * x, axis=1, keepdims=True)
    own = resid_ref.shape[0]
    wide_scr[...] = jnp.where(live, x, 0.0).reshape(wide_scr.shape)
    live_own = jnp.where(live, 1.0, 0.0)
    square_scr[...] = jnp.broadcast_to(live_own, (rows, LANES)).reshape(square_scr.shape)
    rank = lax.axis_index("tp")
    chosen = wide_scr[rank]
    per = square_scr.shape[1] // own
    alive = square_scr[rank // per, pl.ds(pl.multiple_of((rank % per) * own, own), own), 0:1] > 0.5
    resid_ref[...] = jnp.where(alive, chosen, tokens_ref[...].astype(f32))
    project(scaled, squares, weights, keep_ref, send_ref, scaled_scr, square_scr)


def add_kernel(keep_ref, got_ref, own_ref, *send_refs):
    width = own_ref.shape[1] - LANES
    here, size = lax.axis_index("x"), keep_ref.shape[0]
    for shift, target in enumerate((own_ref, *send_refs)):
        x = (here + shift) % size
        total = keep_ref[x] + got_ref[x].astype(f32)
        square = total[:, width:]
        square = square + pltpu.roll(square, LANES // 2, 1)
        target[:, :width] = total[:, :width].astype(target.dtype)
        target[:, width:] = two_lanes(square).astype(target.dtype)


def mix_kernel(steps, block, size, lens_ref, base_ref, gain_ref, state_ref, *refs):
    parts = refs[:size]
    gated_ref, new_ref, rows_scr, seen_scr, value_scr, read_scr = refs[-6:]
    seqs = state_ref.shape[1]
    mask = head_mask()
    total = parts[0][...]
    for part in parts[1:]:
        total = total + part[...].astype(f32)
    square = total[:, 6 * LANES :]
    square = square + pltpu.roll(square, LANES // 2, 1)
    inv_rms = lax.rsqrt(square * (1.0 / D) + norm_eps)
    recept, keys, values, decay_pre, rate_pre, gate_pre = (
        total[:, i * LANES : (i + 1) * LANES] * inv_rms for i in range(6)
    )
    first = lax.axis_index(DP) * seqs
    live = jnp.concatenate(
        [iota((steps, LANES), 0) < lens_ref[first + b] for b in range(seqs)], axis=0
    )
    decay = jnp.exp(-decay_scale * jax.nn.sigmoid(decay_pre + base_ref[block : block + 1]))
    rate = jax.nn.sigmoid(rate_pre)
    unit = keys * lax.rsqrt(head_sum(keys * keys, mask) + key_eps)
    rows_scr[0] = unit
    rows_scr[1] = jnp.where(live, decay, 1.0)
    rows_scr[2] = jnp.where(live, unit * rate, 0.0)
    rows_scr[3] = jnp.where(live, keys, 0.0)
    rows_scr[4] = values
    rows_scr[5] = recept
    diagonal = iota((HEAD, LANES), 0) == iota((HEAD, LANES), 1) % HEAD

    def row(which, b, s):
        return rows_scr[which, pl.ds(b * steps + s, 1), :]

    def widened(s):
        return [jnp.where(diagonal, row(4, b, s), 0.0) for b in range(seqs)]

    left = [state_ref[0, b] * row(0, b, 0) for b in range(seqs)] + widened(0)
    sums = head_sum(jnp.concatenate(left, axis=0), mask)
    span = seqs * HEAD
    seen_scr[...] = sums[:span].reshape(seen_scr.shape)
    value_scr[...] = sums[span:].reshape(value_scr.shape)
    new_ref[0] = state_ref[0]

    def step(s, carry):
        later = jnp.minimum(s + 1, steps - 1)
        ahead, now = [], []
        for b in range(seqs):
            state = (
                new_ref[0, b] * row(1, b, s)
                - seen_scr[b] * row(2, b, s)
                + value_scr[b] * row(3, b, s)
            )
            new_ref[0, b] = state
            ahead.append(state * row(0, b, later))
            now.append(state * row(5, b, s))
        sums = head_sum(jnp.concatenate(now + ahead + widened(later), axis=0), mask)
        for b in range(seqs):
            read = jnp.where(diagonal, sums[b * HEAD : (b + 1) * HEAD], 0.0)
            read_scr[pl.ds(b * steps + s, 1), :] = jnp.sum(read, axis=0, keepdims=True)
        seen_scr[...] = sums[span : 2 * span].reshape(seen_scr.shape)
        value_scr[...] = sums[2 * span :].reshape(value_scr.shape)
        return carry

    lax.fori_loop(0, steps, step, 0)
    read = read_scr[...]
    centered = read - head_sum(read, mask) * (1.0 / HEAD)
    spread = head_sum(centered * centered, mask) * (1.0 / HEAD)
    normed = centered * lax.rsqrt(spread + group_eps)
    gated = normed * gain_ref[block : block + 1] * jax.nn.sigmoid(gate_pre)
    gated = jnp.where(live, gated, 0.0).astype(bf16)
    for d in range(gated_ref.shape[0]):
        gated_ref[d] = gated


def out_compact_kernel(steps, lens_ref, gated_ref, weight_ref, out_ref):
    slots = out_ref.shape[0] * out_ref.shape[1]
    pick = compact_rows(lens_ref[...], slots, gated_ref.shape[0], steps, 0)
    rows = jnp.dot(pick, gated_ref[...], preferred_element_type=f32).astype(bf16)
    part = jnp.dot(rows, weight_ref[0], preferred_element_type=f32)
    out_ref[...] = part.astype(bf16).reshape(out_ref.shape)


def out_kernel(gated_ref, weight_ref, out_ref):
    part = jnp.dot(gated_ref[...], weight_ref[0], preferred_element_type=f32)
    out_ref[...] = part.astype(bf16).reshape(out_ref.shape)


def join_kernel(steps, lens_ref, tokens_ref, parts_ref, gain_ref, out_ref):
    slots = parts_ref.shape[1]
    pick = compact_rows(
        lens_ref[...], slots, tokens_ref.shape[0], steps, lax.axis_index("tp") * slots
    )
    x = jnp.dot(pick, tokens_ref[...], preferred_element_type=f32)
    total = parts_ref[0].astype(f32)
    for t in range(1, parts_ref.shape[0]):
        total = total + parts_ref[t].astype(f32)
    scaled = ((x + total) * gain_ref[1:2]).astype(bf16)
    for t in range(out_ref.shape[0]):
        out_ref[t] = scaled


def final_kernel(parts_ref, resid_ref, out_ref):
    total = parts_ref[0].astype(f32)
    for t in range(1, parts_ref.shape[0]):
        total = total + parts_ref[t].astype(f32)
    out_ref[...] = resid_ref[...] + total


def body(
    tokens,
    lengths,
    norm_gain,
    w_recept,
    w_key,
    w_value,
    w_decay,
    w_rate,
    w_gate,
    w_out,
    decay_base,
    out_gain,
    states,
):
    own_seqs, steps, feats = tokens.shape
    tp, xs = lax.axis_size("tp"), lax.axis_size("x")
    owners = xs * CORES
    own = own_seqs * steps
    rows = own * tp
    held = rows // owners
    seqs = states.shape[1]
    lanes = w_key.shape[2]
    width = 6 * lanes + LANES
    assert lanes == LANES and SLOTS * tp >= LIVE and seqs * steps == held

    lens_row = lengths.reshape(1, -1)
    mine = tokens.reshape(own, feats)
    everyone = lax.all_gather(mine, "tp", axis=0, tiled=True)
    weights = (w_recept, w_key, w_value, w_decay, w_rate, w_gate)

    def pick(block, shape):
        return pl.BlockSpec((1, *shape), lambda _: (block, *(0 for _ in shape)))

    def weight_specs(block):
        return [pick(block, (feats, lanes)) for _ in weights]

    pair = (pltpu.VMEM((xs, held, width), f32), pltpu.VMEM((xs, held, width), bf16))
    project_scratch = (
        pltpu.VMEM((owners, held, feats), bf16),
        pltpu.VMEM((owners, held, LANES), f32),
    )

    def exchange(keep, send):
        got = lax.ppermute(send, "c", [(0, 1), (1, 0)])
        block = (held, width)
        own_part, *sends = call(
            add_kernel,
            (pltpu.VMEM(block, f32), *(pltpu.VMEM(block, bf16) for _ in range(1, xs))),
            [vmem(), vmem()],
        )(near(keep), near(got))
        return [own_part] + [
            lax.ppermute(send, "x", [(i, (i + shift) % xs) for i in range(xs)])
            for shift, send in enumerate(sends, 1)
        ]

    def mixed(block, parts, news):
        out_shape = (
            pltpu.VMEM((owners, held, lanes), bf16),
            jax.ShapeDtypeStruct(states.shape, f32),
        )
        extra = [] if news is None else [news]
        gated, news = call(
            functools.partial(mix_kernel, steps, block, xs),
            out_shape,
            [smem(), vmem(), vmem(), pick(block, states.shape[1:])]
            + [vmem()] * xs
            + [pl.BlockSpec(memory_space=pl.ANY)] * len(extra),
            (vmem(), pick(block, states.shape[1:])),
            (
                pltpu.VMEM((6, held, LANES), f32),
                pltpu.VMEM((seqs, HEAD, LANES), f32),
                pltpu.VMEM((seqs, HEAD, LANES), f32),
                pltpu.VMEM((held, LANES), f32),
            ),
            input_output_aliases={4 + xs: 1} if extra else {},
        )(
            lengths,
            decay_base,
            out_gain,
            states,
            *(near(part) for part in parts),
            *extra,
        )
        gathered = lax.all_to_all(gated, DP, 0, 0, tiled=True)
        return gathered.reshape(rows, lanes), news

    keep, send = call(
        first_kernel,
        pair,
        [vmem(), vmem(), *weight_specs(0)],
        scratch=project_scratch,
    )(near(everyone), norm_gain, *weights)
    gated, news = mixed(0, exchange(keep, send), None)
    partial = call(
        functools.partial(out_compact_kernel, steps),
        pltpu.VMEM((tp, SLOTS, feats), bf16),
        [vmem(), vmem(), pick(0, (lanes, feats))],
    )(lens_row, near(gated), w_out)
    partial = lax.all_to_all(partial, "tp", 0, 0, tiled=True)
    scaled = call(
        functools.partial(join_kernel, steps),
        pltpu.VMEM((tp, SLOTS, feats), bf16),
        [vmem(), vmem(), vmem(), vmem()],
    )(lens_row, near(everyone), near(partial), norm_gain)
    scaled = lax.all_to_all(scaled, "tp", 0, 0, tiled=True).reshape(tp * SLOTS, feats)
    keep, send, resid = call(
        functools.partial(next_kernel, steps),
        (*pair, pltpu.VMEM((own, feats), f32)),
        [vmem(), vmem(), vmem(), vmem(), *weight_specs(1)],
        scratch=(*project_scratch, pltpu.VMEM((tp, own, feats), f32)),
    )(lens_row, near(scaled), mine, norm_gain, *weights)
    gated, news = mixed(1, exchange(keep, send), news)
    partial = call(
        out_kernel,
        pltpu.VMEM((tp, own, feats), bf16),
        [vmem(), pick(1, (lanes, feats))],
    )(near(gated), w_out)
    partial = lax.all_to_all(partial, "tp", 0, 0, tiled=True)
    stream = call(final_kernel, jax.ShapeDtypeStruct((own, feats), f32), [vmem(), vmem()])(
        near(partial), near(resid)
    )
    return stream.reshape(tokens.shape), news


def solution(mesh):
    split = Mesh(
        mesh.devices.reshape(
            mesh.shape["grp"], mesh.shape["tp"], mesh.shape["dp"] // CORES, CORES
        ),
        ("grp", "tp", "x", "c"),
    )
    return jax.shard_map(
        body,
        mesh=split,
        in_specs=(
            P(("grp", "tp"), None, DP),
            P("grp"),
            P(None, DP),
            P(None, DP, "tp"),
            P(None, DP, "tp"),
            P(None, DP, "tp"),
            P(None, DP, "tp"),
            P(None, DP, "tp"),
            P(None, DP, "tp"),
            P(None, "tp", DP),
            P(None, "tp"),
            P(None, "tp"),
            P(None, GRP_DP, None, "tp"),
        ),
        out_specs=(P(("grp", "tp"), None, DP), P(None, GRP_DP, None, "tp")),
        check_vma=False,
    )
```

```python
import functools

import jax
import jax.numpy as jnp
from jax import lax
from jax.experimental import pallas as pl
from jax.experimental.pallas import tpu as pltpu
from jax.sharding import Mesh
from jax.sharding import PartitionSpec as P

D = 4096
HEAD = 64
BLOCKS = 2
LANES = 128
CORES = 2
PAIR = 2
LIVE = 224
SLOTS = 16
DP = ("x", "c")
TP = ("th", "tl")
GRP_DP = ("grp", "x", "c")

group_eps = 0.00064
norm_eps = 1e-06
key_eps = 1e-06
decay_scale = 0.606531


f32 = jnp.float32
bf16 = jnp.bfloat16


def iota(shape, dim):
    return lax.broadcasted_iota(jnp.int32, shape, dim)


def vmem():
    return pl.BlockSpec(memory_space=pltpu.VMEM)


def smem():
    return pl.BlockSpec(memory_space=pltpu.SMEM)


def near(value):
    return pltpu.with_memory_space_constraint(value, pltpu.VMEM)


def call(kernel, out_shape, in_specs, out_specs=None, scratch=(), **more):
    if out_specs is None:
        out_specs = tuple(vmem() for _ in out_shape) if isinstance(out_shape, tuple) else vmem()
    return pl.pallas_call(
        kernel,
        grid=(1,),
        out_shape=out_shape,
        in_specs=in_specs,
        out_specs=out_specs,
        scratch_shapes=list(scratch),
        compiler_params=pltpu.CompilerParams(vmem_limit_bytes=24 * 2**20),
        **more,
    )


def halves(value):
    high = value.astype(bf16)
    return high, (value - high.astype(f32)).astype(bf16)


def split_two(value):
    return jnp.concatenate(halves(value), axis=1)


def head_mask():
    rows, cols = iota((2 * LANES, LANES), 0), iota((2 * LANES, LANES), 1)
    return jnp.where((rows % LANES) // HEAD == cols // HEAD, 1.0, 0.0).astype(bf16)


def head_sum(value, mask):
    return jnp.dot(split_two(value), mask, preferred_element_type=f32)


def compact_rows(lens, slots, rows, steps, first):
    seqs = rows // steps
    seq_of = iota((seqs, rows), 1) // steps
    before = jnp.where(iota((seqs, rows), 0) < seq_of, 1.0, 0.0).astype(bf16)
    same = jnp.where(iota((seqs, rows), 0) == seq_of, 1.0, 0.0).astype(bf16)
    wide = jnp.broadcast_to(lens.astype(f32), (8, seqs)).astype(bf16)
    start = jnp.dot(wide, before, preferred_element_type=f32)[0:1]
    count = jnp.dot(wide, same, preferred_element_type=f32)[0:1]
    step = (iota((1, rows), 1) % steps).astype(f32)
    place = jnp.where(step < count, start + step, -1.0)
    slot = (iota((slots, rows), 0) + first).astype(f32)
    return jnp.where(slot == jnp.broadcast_to(place, (slots, rows)), 1.0, 0.0).astype(bf16)


def spread_rows(lens, rows, slots, steps):
    seqs = rows // steps
    wide = jnp.broadcast_to(lens.astype(f32), (rows, seqs))
    seq_of = iota((rows, seqs), 0) // steps
    start = jnp.sum(jnp.where(iota((rows, seqs), 1) < seq_of, wide, 0.0), axis=1, keepdims=True)
    count = jnp.sum(jnp.where(iota((rows, seqs), 1) == seq_of, wide, 0.0), axis=1, keepdims=True)
    step = (iota((rows, 1), 0) % steps).astype(f32)
    live = step < count
    place = jnp.where(live, start + step, -1.0)
    slot = iota((rows, slots), 1).astype(f32)
    return jnp.where(slot == jnp.broadcast_to(place, (rows, slots)), 1.0, 0.0).astype(bf16), live


def two_lanes(total):
    high = total.astype(bf16).astype(f32)
    return jnp.where(iota(total.shape, 1) < LANES // 2, high, total - high)


def project(weights, keep_ref, send_ref, scaled_scr, square_scr):
    owners = scaled_scr.shape[0]
    held = scaled_scr.shape[1]
    weight = jnp.concatenate([w[0] for w in weights], axis=1)
    width = weight.shape[1]
    core = lax.axis_index("c")
    for target, who in ((send_ref, 1 - core), (keep_ref, core)):
        left = jnp.concatenate([scaled_scr[CORES * x + who] for x in range(owners // CORES)], axis=0)
        part = jnp.dot(left, weight, preferred_element_type=f32)
        for x in range(owners // CORES):
            target[x, :, :width] = part[x * held : (x + 1) * held].astype(target.dtype)
            square = square_scr[CORES * x + who]
            if target is send_ref:
                square = two_lanes(square)
            else:
                square = jnp.where(iota(square.shape, 1) < LANES // 2, square, 0.0)
            target[x, :, width:] = square.astype(target.dtype)


def first_kernel(tokens_ref, gain_ref, *refs):
    weights, (keep_ref, send_ref, scaled_scr, square_scr) = refs[:6], refs[6:]
    x = tokens_ref[...].astype(f32)
    scaled_scr[...] = (x * gain_ref[0:1]).astype(bf16).reshape(scaled_scr.shape)
    squares = jnp.sum(x * x, axis=1, keepdims=True)
    square_scr[...] = jnp.broadcast_to(squares, (x.shape[0], LANES)).reshape(square_scr.shape)
    project(weights, keep_ref, send_ref, scaled_scr, square_scr)


def next_kernel(steps, lens_ref, near_ref, far_ref, tokens_ref, gain_ref, *refs):
    weights = refs[:6]
    keep_ref, send_ref, resid_ref, scaled_scr, square_scr, wide_scr, slot_scr = refs[6:]
    rows = scaled_scr.shape[0] * scaled_scr.shape[1]
    side = lax.axis_index("tl")
    for half_ref, place in ((near_ref, side), (far_ref, 1 - side)):
        slot_scr[:, place] = half_ref[...]
    slots = slot_scr[...].reshape(-1, slot_scr.shape[3])
    spread, live = spread_rows(lens_ref[...], rows, slots.shape[0], steps)
    wide = jnp.dot(spread, slots, preferred_element_type=f32)
    scaled_scr[...] = wide.astype(bf16).reshape(scaled_scr.shape)
    x = wide * (1.0 / gain_ref[1:2])
    squares = jnp.sum(x * x, axis=1, keepdims=True)
    own = resid_ref.shape[0]
    wide_scr[...] = x.reshape(wide_scr.shape)
    square_scr[...] = jnp.broadcast_to(jnp.where(live, 1.0, 0.0), (rows, LANES)).reshape(
        square_scr.shape
    )
    rank = lax.axis_index(TP)
    per = square_scr.shape[1] // own
    alive = square_scr[rank // per, pl.ds(pl.multiple_of((rank % per) * own, own), own), 0:1] > 0.5
    resid_ref[...] = jnp.where(alive, wide_scr[rank], tokens_ref[...].astype(f32))
    square_scr[...] = jnp.broadcast_to(squares, (rows, LANES)).reshape(square_scr.shape)
    project(weights, keep_ref, send_ref, scaled_scr, square_scr)


def add_kernel(keep_ref, got_ref, own_ref, *send_refs):
    width = own_ref.shape[1] - LANES
    here, size = lax.axis_index("x"), keep_ref.shape[0]
    for shift, target in enumerate((own_ref, *send_refs)):
        x = (here + shift) % size
        total = keep_ref[x] + got_ref[x].astype(f32)
        square = total[:, width:]
        square = square + pltpu.roll(square, LANES // 2, 1)
        target[:, :width] = total[:, :width].astype(target.dtype)
        target[:, width:] = two_lanes(square).astype(target.dtype)


def mix_kernel(steps, block, size, lens_ref, base_ref, gain_ref, state_ref, *refs):
    parts = refs[:size]
    gated_ref, new_ref = refs[-2:]
    seqs = state_ref.shape[1]
    mask = head_mask()
    total = parts[0][...]
    for part in parts[1:]:
        total = total + part[...].astype(f32)
    square = total[:, 6 * LANES :]
    square = square + pltpu.roll(square, LANES // 2, 1)
    inv_rms = lax.rsqrt(square * (1.0 / D) + norm_eps)
    recept, keys, values, decay_pre, rate_pre, gate_pre = (
        total[:, i * LANES : (i + 1) * LANES] * inv_rms for i in range(6)
    )
    first = lax.axis_index(DP) * seqs
    live = jnp.concatenate(
        [iota((steps, LANES), 0) < lens_ref[first + b] for b in range(seqs)], axis=0
    )
    fall = -decay_scale * jax.nn.sigmoid(decay_pre + base_ref[block : block + 1])
    fall = jnp.where(live, fall, 0.0)
    rate = jax.nn.sigmoid(rate_pre)
    unit = keys * lax.rsqrt(head_sum(keys * keys, mask) + key_eps)
    removal = jnp.where(live, unit * rate, 0.0)
    keys = jnp.where(live, keys, 0.0)
    rows = unit.shape[0]
    position = iota((rows, LANES), 0) % steps

    def row(value, s):
        value = value.reshape(seqs, steps, LANES)[:, s : s + 1]
        return jnp.broadcast_to(value, (seqs, steps, LANES)).reshape(rows, LANES)

    def cut(value, b):
        return value[b * steps : (b + 1) * steps]

    until, reach = fall, 1
    while reach < steps:
        until = until + jnp.where(position >= reach, pltpu.roll(until, reach, 0), 0.0)
        reach *= 2
    before = until - fall

    products = []
    for s in range(steps):
        until_s, keys_s, removal_s = row(until, s), row(keys, s), row(removal, s)
        seeing = jnp.where(position > s, unit * jnp.exp(before - until_s), 0.0)
        reading = jnp.where(position >= s, recept * jnp.exp(until - until_s), 0.0)
        products += [seeing * keys_s, seeing * removal_s, reading * keys_s, reading * removal_s]
    sums = head_sum(jnp.concatenate(products, axis=0), mask)
    pairs = [sums[i * rows : (i + 1) * rows] for i in range(4 * steps)]

    seeing, reading = unit * jnp.exp(before), recept * jnp.exp(until)
    lane = iota((HEAD, LANES), 1) < HEAD
    seen, read = [], []
    for b in range(seqs):
        left = jnp.concatenate([cut(seeing, b), cut(reading, b)], axis=0)
        high, low = halves(left)
        left = jnp.concatenate([high, low, high], axis=1)
        state = state_ref[0, b]
        high, low = halves(
            jnp.concatenate([jnp.where(lane, state, 0.0), jnp.where(lane, 0.0, state)], axis=0)
        )
        right = jnp.concatenate([high, high, low], axis=1)
        part = lax.dot_general(
            left, right, (((1,), (1,)), ((), ())), preferred_element_type=f32
        )
        seen.append(part[:steps])
        read.append(part[steps:])
    seen, read = jnp.concatenate(seen, axis=0), jnp.concatenate(read, axis=0)
    for s in range(steps):
        values_s = row(values, s)
        seen = seen + pairs[4 * s] * values_s
        read = read + pairs[4 * s + 2] * values_s
    for s in range(steps):
        seen_s = row(seen, s)
        seen = seen - pairs[4 * s + 1] * seen_s
        read = read - pairs[4 * s + 3] * seen_s

    last = row(until, steps - 1)
    onward = jnp.exp(last - until)
    keys, removal, last = keys * onward, removal * onward, jnp.exp(last)
    for b in range(seqs):
        high, low = halves(jnp.concatenate([cut(values, b), -cut(seen, b)], axis=0))
        left = jnp.concatenate([high, low, high], axis=0)
        high, low = halves(jnp.concatenate([cut(keys, b), cut(removal, b)], axis=0))
        right = jnp.concatenate([high, high, low], axis=0)
        part = lax.dot_general(
            left, right, (((0,), (0,)), ((), ())), preferred_element_type=f32
        )
        part = jnp.where(lane, part[:HEAD], part[HEAD:])
        new_ref[0, b] = state_ref[0, b] * last[b * steps : b * steps + 1] + part
    centered = read - head_sum(read, mask) * (1.0 / HEAD)
    spread = head_sum(centered * centered, mask) * (1.0 / HEAD)
    normed = centered * lax.rsqrt(spread + group_eps)
    gated = normed * gain_ref[block : block + 1] * jax.nn.sigmoid(gate_pre)
    gated = jnp.where(live, gated, 0.0).astype(bf16)
    for d in range(gated_ref.shape[0]):
        gated_ref[d] = gated


def halve(part, keep_ref, send_ref, scr):
    side = lax.axis_index("tl")
    scr[...] = part.reshape(scr.shape)
    keep_ref[...] = scr[:, side]
    send_ref[...] = scr[:, 1 - side].astype(bf16)


def out_compact_kernel(steps, lens_ref, gated_ref, weight_ref, keep_ref, send_ref, scr):
    slots = scr.shape[0] * scr.shape[1] * scr.shape[2]
    pick = compact_rows(lens_ref[...], slots, gated_ref.shape[0], steps, 0)
    rows = jnp.dot(pick, gated_ref[...], preferred_element_type=f32).astype(bf16)
    halve(jnp.dot(rows, weight_ref[0], preferred_element_type=f32), keep_ref, send_ref, scr)


def out_kernel(gated_ref, weight_ref, keep_ref, send_ref, scr):
    part = jnp.dot(gated_ref[...], weight_ref[0], preferred_element_type=f32)
    halve(part, keep_ref, send_ref, scr)


def pair_kernel(keep_ref, got_ref, out_ref):
    out_ref[...] = (keep_ref[...] + got_ref[...].astype(f32)).astype(bf16)


def sum_parts(parts_ref):
    total = parts_ref[0].astype(f32)
    for t in range(1, parts_ref.shape[0]):
        total = total + parts_ref[t].astype(f32)
    return total


def join_kernel(steps, lens_ref, tokens_ref, parts_ref, gain_ref, out_ref):
    slots = parts_ref.shape[1]
    pick = compact_rows(
        lens_ref[...], slots, tokens_ref.shape[0], steps, lax.axis_index(TP) * slots
    )
    x = jnp.dot(pick, tokens_ref[...], preferred_element_type=f32)
    scaled = ((x + sum_parts(parts_ref)) * gain_ref[1:2]).astype(bf16)
    for t in range(out_ref.shape[0]):
        out_ref[t] = scaled


def final_kernel(parts_ref, resid_ref, out_ref):
    out_ref[...] = resid_ref[...] + sum_parts(parts_ref)


def body(
    tokens,
    lengths,
    norm_gain,
    w_recept,
    w_key,
    w_value,
    w_decay,
    w_rate,
    w_gate,
    w_out,
    decay_base,
    out_gain,
    states,
):
    own_seqs, steps, feats = tokens.shape
    th, xs = lax.axis_size("th"), lax.axis_size("x")
    tp = th * PAIR
    owners = xs * CORES
    own = own_seqs * steps
    rows = own * tp
    held = rows // owners
    seqs = states.shape[1]
    lanes = w_key.shape[2]
    width = 6 * lanes + LANES
    assert lanes == LANES and SLOTS * tp >= LIVE and seqs * steps == held

    lens_row = lengths.reshape(1, -1)
    mine = tokens.reshape(own, feats)
    weights = (w_recept, w_key, w_value, w_decay, w_rate, w_gate)

    def pick(block, shape):
        return pl.BlockSpec((1, *shape), lambda _: (block, *(0 for _ in shape)))

    def weight_specs(block):
        return [pick(block, (feats, lanes)) for _ in weights]

    pair = (pltpu.VMEM((xs, held, width), f32), pltpu.VMEM((xs, held, width), bf16))
    project_scratch = (
        pltpu.VMEM((owners, held, feats), bf16),
        pltpu.VMEM((owners, held, LANES), f32),
    )

    def exchange(keep, send):
        got = lax.ppermute(send, "c", swap)
        block = (held, width)
        own_part, *sends = call(
            add_kernel,
            (pltpu.VMEM(block, f32), *(pltpu.VMEM(block, bf16) for _ in range(1, xs))),
            [vmem(), vmem()],
        )(near(keep), near(got))
        return [own_part] + [
            lax.ppermute(send, "x", [(i, (i + shift) % xs) for i in range(xs)])
            for shift, send in enumerate(sends, 1)
        ]

    def mixed(block, parts, news):
        out_shape = (
            pltpu.VMEM((owners, held, lanes), bf16),
            jax.ShapeDtypeStruct(states.shape, f32),
        )
        extra = [] if news is None else [news]
        gated, news = call(
            functools.partial(mix_kernel, steps, block, xs),
            out_shape,
            [smem(), vmem(), vmem(), pick(block, states.shape[1:])]
            + [vmem()] * xs
            + [pl.BlockSpec(memory_space=pl.ANY)] * len(extra),
            (vmem(), pick(block, states.shape[1:])),
            input_output_aliases={4 + xs: 1} if extra else {},
        )(
            lengths,
            decay_base,
            out_gain,
            states,
            *(near(part) for part in parts),
            *extra,
        )
        gathered = lax.all_to_all(gated, DP, 0, 0, tiled=True)
        return gathered.reshape(rows, lanes), news

    swap = [(0, 1), (1, 0)]

    def gather(value):
        near_half = lax.all_to_all(value, "th", 0, 0, tiled=True)
        return near(near_half), near(lax.ppermute(near_half, "tl", swap))

    def scatter(kernel, count, specs, *args):
        block = (th, count, feats)
        keep, send = call(
            kernel,
            (pltpu.VMEM(block, f32), pltpu.VMEM(block, bf16)),
            specs,
            scratch=(pltpu.VMEM((th, PAIR, count, feats), f32),),
        )(*args)
        got = lax.ppermute(send, "tl", swap)
        both = call(pair_kernel, pltpu.VMEM(block, bf16), [vmem(), vmem()])(near(keep), near(got))
        return near(lax.all_to_all(both, "th", 0, 0, tiled=True))

    everyone = near(lax.all_gather(mine, TP, axis=0, tiled=True))
    keep, send = call(
        first_kernel, pair, [vmem(), vmem(), *weight_specs(0)], scratch=project_scratch
    )(everyone, norm_gain, *(pltpu.with_memory_space_constraint(w, pltpu.HBM) for w in weights))
    gated, news = mixed(0, exchange(keep, send), None)
    partial = scatter(
        functools.partial(out_compact_kernel, steps),
        SLOTS,
        [vmem(), vmem(), pick(0, (lanes, feats))],
        lens_row,
        near(gated),
        w_out,
    )
    scaled = call(
        functools.partial(join_kernel, steps),
        pltpu.VMEM((th, SLOTS, feats), bf16),
        [vmem(), vmem(), vmem(), vmem()],
    )(lens_row, everyone, partial, norm_gain)
    keep, send, resid = call(
        functools.partial(next_kernel, steps),
        (*pair, pltpu.VMEM((own, feats), f32)),
        [vmem(), vmem(), vmem(), vmem(), vmem(), *weight_specs(1)],
        scratch=(
            *project_scratch,
            pltpu.VMEM((tp, own, feats), f32),
            pltpu.VMEM((th, PAIR, SLOTS, feats), bf16),
        ),
    )(lens_row, *gather(scaled), mine, norm_gain, *weights)
    gated, news = mixed(1, exchange(keep, send), news)
    partial = scatter(out_kernel, own, [vmem(), pick(1, (lanes, feats))], near(gated), w_out)
    stream = call(final_kernel, jax.ShapeDtypeStruct((own, feats), f32), [vmem(), vmem()])(
        partial, near(resid)
    )
    return stream.reshape(tokens.shape), news


def solution(mesh):
    split = Mesh(
        mesh.devices.reshape(
            mesh.shape["grp"],
            mesh.shape["tp"] // PAIR,
            PAIR,
            mesh.shape["dp"] // CORES,
            CORES,
        ),
        ("grp", "th", "tl", "x", "c"),
    )
    return jax.shard_map(
        body,
        mesh=split,
        in_specs=(
            P(("grp", *TP), None, DP),
            P("grp"),
            P(None, DP),
            P(None, DP, TP),
            P(None, DP, TP),
            P(None, DP, TP),
            P(None, DP, TP),
            P(None, DP, TP),
            P(None, DP, TP),
            P(None, TP, DP),
            P(None, TP),
            P(None, TP),
            P(None, GRP_DP, None, TP),
        ),
        out_specs=(P(("grp", *TP), None, DP), P(None, GRP_DP, None, TP)),
        check_vma=False,
    )
```

```python
import functools

import jax
import jax.numpy as jnp
from jax import lax
from jax.experimental import pallas as pl
from jax.experimental.pallas import tpu as pltpu
from jax.sharding import Mesh
from jax.sharding import PartitionSpec as P

D = 4096
HEAD = 64
BLOCKS = 2
LANES = 128
CORES = 2
PAIR = 2
QUAD = 4
LIVE = 224
SLOTS = 16
DP = ("x", "c")
TP = ("ta", "tm", "tl")
TH = ("ta", "tm")
TQ = ("tm", "tl")
GRP_DP = ("grp", "x", "c")

group_eps = 0.00064
norm_eps = 1e-06
key_eps = 1e-06
decay_scale = 0.606531


f32 = jnp.float32
bf16 = jnp.bfloat16


def iota(shape, dim):
    return lax.broadcasted_iota(jnp.int32, shape, dim)


def vmem():
    return pl.BlockSpec(memory_space=pltpu.VMEM)


def smem():
    return pl.BlockSpec(memory_space=pltpu.SMEM)


def near(value):
    return pltpu.with_memory_space_constraint(value, pltpu.VMEM)


def call(kernel, out_shape, in_specs, out_specs=None, scratch=(), **more):
    if out_specs is None:
        out_specs = tuple(vmem() for _ in out_shape) if isinstance(out_shape, tuple) else vmem()
    return pl.pallas_call(
        kernel,
        grid=(1,),
        out_shape=out_shape,
        in_specs=in_specs,
        out_specs=out_specs,
        scratch_shapes=list(scratch),
        compiler_params=pltpu.CompilerParams(vmem_limit_bytes=24 * 2**20),
        **more,
    )


def halves(value):
    high = value.astype(bf16)
    return high, (value - high.astype(f32)).astype(bf16)


def split_two(value):
    return jnp.concatenate(halves(value), axis=1)


def head_mask():
    rows, cols = iota((2 * LANES, LANES), 0), iota((2 * LANES, LANES), 1)
    return jnp.where((rows % LANES) // HEAD == cols // HEAD, 1.0, 0.0).astype(bf16)


def head_sum(value, mask):
    return jnp.dot(split_two(value), mask, preferred_element_type=f32)


def compact_rows(lens, slots, rows, steps, first):
    seqs = rows // steps
    seq_of = iota((seqs, rows), 1) // steps
    before = jnp.where(iota((seqs, rows), 0) < seq_of, 1.0, 0.0).astype(bf16)
    same = jnp.where(iota((seqs, rows), 0) == seq_of, 1.0, 0.0).astype(bf16)
    wide = jnp.broadcast_to(lens.astype(f32), (8, seqs)).astype(bf16)
    start = jnp.dot(wide, before, preferred_element_type=f32)[0:1]
    count = jnp.dot(wide, same, preferred_element_type=f32)[0:1]
    step = (iota((1, rows), 1) % steps).astype(f32)
    place = jnp.where(step < count, start + step, -1.0)
    slot = (iota((slots, rows), 0) + first).astype(f32)
    return jnp.where(slot == jnp.broadcast_to(place, (slots, rows)), 1.0, 0.0).astype(bf16)


def spread_rows(lens, rows, slots, steps):
    seqs = rows // steps
    wide = jnp.broadcast_to(lens.astype(f32), (rows, seqs))
    seq_of = iota((rows, seqs), 0) // steps
    start = jnp.sum(jnp.where(iota((rows, seqs), 1) < seq_of, wide, 0.0), axis=1, keepdims=True)
    count = jnp.sum(jnp.where(iota((rows, seqs), 1) == seq_of, wide, 0.0), axis=1, keepdims=True)
    step = (iota((rows, 1), 0) % steps).astype(f32)
    live = step < count
    place = jnp.where(live, start + step, -1.0)
    slot = iota((rows, slots), 1).astype(f32)
    return jnp.where(slot == jnp.broadcast_to(place, (rows, slots)), 1.0, 0.0).astype(bf16), live


def two_lanes(total):
    high = total.astype(bf16).astype(f32)
    return jnp.where(iota(total.shape, 1) < LANES // 2, high, total - high)


def project(weights, keep_ref, send_ref, scaled_scr, square_scr):
    owners = scaled_scr.shape[0]
    held = scaled_scr.shape[1]
    weight = jnp.concatenate([w[0] for w in weights], axis=1)
    width = weight.shape[1]
    core = lax.axis_index("c")
    for target, who in ((send_ref, 1 - core), (keep_ref, core)):
        left = jnp.concatenate([scaled_scr[CORES * x + who] for x in range(owners // CORES)], axis=0)
        part = jnp.dot(left, weight, preferred_element_type=f32)
        for x in range(owners // CORES):
            target[x, :, :width] = part[x * held : (x + 1) * held].astype(target.dtype)
            square = square_scr[CORES * x + who]
            if target is send_ref:
                square = two_lanes(square)
            else:
                square = jnp.where(iota(square.shape, 1) < LANES // 2, square, 0.0)
            target[x, :, width:] = square.astype(target.dtype)


def first_kernel(tokens_ref, gain_ref, *refs):
    weights, (keep_ref, send_ref, scaled_scr, square_scr) = refs[:6], refs[6:]
    x = tokens_ref[...].astype(f32)
    scaled_scr[...] = (x * gain_ref[0:1]).astype(bf16).reshape(scaled_scr.shape)
    squares = jnp.sum(x * x, axis=1, keepdims=True)
    square_scr[...] = jnp.broadcast_to(squares, (x.shape[0], LANES)).reshape(square_scr.shape)
    project(weights, keep_ref, send_ref, scaled_scr, square_scr)


def next_kernel(steps, lens_ref, near_ref, far_ref, tokens_ref, gain_ref, *refs):
    weights = refs[:6]
    keep_ref, send_ref, resid_ref, scaled_scr, square_scr, wide_scr, slot_scr = refs[6:]
    rows = scaled_scr.shape[0] * scaled_scr.shape[1]
    side = lax.axis_index("tl")
    for half_ref, place in ((near_ref, side), (far_ref, 1 - side)):
        slot_scr[:, place] = half_ref[...]
    slots = slot_scr[...].reshape(-1, slot_scr.shape[3])
    spread, live = spread_rows(lens_ref[...], rows, slots.shape[0], steps)
    wide = jnp.dot(spread, slots, preferred_element_type=f32)
    scaled_scr[...] = wide.astype(bf16).reshape(scaled_scr.shape)
    x = wide * (1.0 / gain_ref[1:2])
    squares = jnp.sum(x * x, axis=1, keepdims=True)
    own = resid_ref.shape[0]
    wide_scr[...] = x.reshape(wide_scr.shape)
    square_scr[...] = jnp.broadcast_to(jnp.where(live, 1.0, 0.0), (rows, LANES)).reshape(
        square_scr.shape
    )
    rank = lax.axis_index(TP)
    per = square_scr.shape[1] // own
    alive = square_scr[rank // per, pl.ds(pl.multiple_of((rank % per) * own, own), own), 0:1] > 0.5
    resid_ref[...] = jnp.where(alive, wide_scr[rank], tokens_ref[...].astype(f32))
    square_scr[...] = jnp.broadcast_to(squares, (rows, LANES)).reshape(square_scr.shape)
    project(weights, keep_ref, send_ref, scaled_scr, square_scr)


def add_kernel(keep_ref, got_ref, own_ref, *send_refs):
    width = own_ref.shape[1] - LANES
    here, size = lax.axis_index("x"), keep_ref.shape[0]
    for shift, target in enumerate((own_ref, *send_refs)):
        x = (here + shift) % size
        total = keep_ref[x] + got_ref[x].astype(f32)
        square = total[:, width:]
        square = square + pltpu.roll(square, LANES // 2, 1)
        target[:, :width] = total[:, :width].astype(target.dtype)
        target[:, width:] = two_lanes(square).astype(target.dtype)


def mix_kernel(steps, block, size, lens_ref, base_ref, gain_ref, state_ref, *refs):
    parts = refs[:size]
    gated_ref, new_ref = refs[-2:]
    seqs = state_ref.shape[1]
    mask = head_mask()
    total = parts[0][...]
    for part in parts[1:]:
        total = total + part[...].astype(f32)
    square = total[:, 6 * LANES :]
    square = square + pltpu.roll(square, LANES // 2, 1)
    inv_rms = lax.rsqrt(square * (1.0 / D) + norm_eps)
    recept, keys, values, decay_pre, rate_pre, gate_pre = (
        total[:, i * LANES : (i + 1) * LANES] * inv_rms for i in range(6)
    )
    first = lax.axis_index(DP) * seqs
    live = jnp.concatenate(
        [iota((steps, LANES), 0) < lens_ref[first + b] for b in range(seqs)], axis=0
    )
    fall = -decay_scale * jax.nn.sigmoid(decay_pre + base_ref[block : block + 1])
    fall = jnp.where(live, fall, 0.0)
    rate = jax.nn.sigmoid(rate_pre)
    unit = keys * lax.rsqrt(head_sum(keys * keys, mask) + key_eps)
    removal = jnp.where(live, unit * rate, 0.0)
    keys = jnp.where(live, keys, 0.0)
    rows = unit.shape[0]
    position = iota((rows, LANES), 0) % steps

    def row(value, s):
        value = value.reshape(seqs, steps, LANES)[:, s : s + 1]
        return jnp.broadcast_to(value, (seqs, steps, LANES)).reshape(rows, LANES)

    def cut(value, b):
        return value[b * steps : (b + 1) * steps]

    until, reach = fall, 1
    while reach < steps:
        until = until + jnp.where(position >= reach, pltpu.roll(until, reach, 0), 0.0)
        reach *= 2
    before = until - fall

    products = []
    for s in range(steps):
        until_s, keys_s, removal_s = row(until, s), row(keys, s), row(removal, s)
        seeing = jnp.where(position > s, unit * jnp.exp(before - until_s), 0.0)
        reading = jnp.where(position >= s, recept * jnp.exp(until - until_s), 0.0)
        products += [seeing * keys_s, seeing * removal_s, reading * keys_s, reading * removal_s]
    sums = head_sum(jnp.concatenate(products, axis=0), mask)
    pairs = [sums[i * rows : (i + 1) * rows] for i in range(4 * steps)]

    seeing, reading = unit * jnp.exp(before), recept * jnp.exp(until)
    lane = iota((HEAD, LANES), 1) < HEAD
    seen, read = [], []
    for b in range(seqs):
        left = jnp.concatenate([cut(seeing, b), cut(reading, b)], axis=0)
        high, low = halves(left)
        left = jnp.concatenate([high, low, high], axis=1)
        state = state_ref[0, b]
        high, low = halves(
            jnp.concatenate([jnp.where(lane, state, 0.0), jnp.where(lane, 0.0, state)], axis=0)
        )
        right = jnp.concatenate([high, high, low], axis=1)
        part = lax.dot_general(
            left, right, (((1,), (1,)), ((), ())), preferred_element_type=f32
        )
        seen.append(part[:steps])
        read.append(part[steps:])
    seen, read = jnp.concatenate(seen, axis=0), jnp.concatenate(read, axis=0)
    for s in range(steps):
        values_s = row(values, s)
        seen = seen + pairs[4 * s] * values_s
        read = read + pairs[4 * s + 2] * values_s
    for s in range(steps):
        seen_s = row(seen, s)
        seen = seen - pairs[4 * s + 1] * seen_s
        read = read - pairs[4 * s + 3] * seen_s

    last = row(until, steps - 1)
    onward = jnp.exp(last - until)
    keys, removal, last = keys * onward, removal * onward, jnp.exp(last)
    for b in range(seqs):
        high, low = halves(jnp.concatenate([cut(values, b), -cut(seen, b)], axis=0))
        left = jnp.concatenate([high, low, high], axis=0)
        high, low = halves(jnp.concatenate([cut(keys, b), cut(removal, b)], axis=0))
        right = jnp.concatenate([high, high, low], axis=0)
        part = lax.dot_general(
            left, right, (((0,), (0,)), ((), ())), preferred_element_type=f32
        )
        part = jnp.where(lane, part[:HEAD], part[HEAD:])
        new_ref[0, b] = state_ref[0, b] * last[b * steps : b * steps + 1] + part
    centered = read - head_sum(read, mask) * (1.0 / HEAD)
    spread = head_sum(centered * centered, mask) * (1.0 / HEAD)
    normed = centered * lax.rsqrt(spread + group_eps)
    gated = normed * gain_ref[block : block + 1] * jax.nn.sigmoid(gate_pre)
    gated = jnp.where(live, gated, 0.0).astype(bf16)
    for d in range(gated_ref.shape[0]):
        gated_ref[d] = gated


def halve(rows, keep_ref, send_ref, scr):
    side = lax.axis_index("tl")
    scr[...] = rows.reshape(scr.shape)
    keep_ref[...] = scr[:, side]
    send_ref[...] = scr[:, 1 - side]


def pick_kernel(steps, lens_ref, gated_ref, keep_ref, send_ref, scr):
    slots = scr.shape[0] * scr.shape[1] * scr.shape[2]
    pick = compact_rows(lens_ref[...], slots, gated_ref.shape[0], steps, 0)
    rows = jnp.dot(pick, gated_ref[...], preferred_element_type=f32).astype(bf16)
    halve(rows, keep_ref, send_ref, scr)


def group_kernel(gated_ref, out_ref):
    places, groups, own, _ = out_ref.shape
    for place in range(places):
        for group in range(groups):
            first = (group * places + place) * own
            out_ref[place, group] = gated_ref[first : first + own]


def last_kernel(got_ref, *refs):
    weights, out_ref = refs[:-1], refs[-1]
    place = lax.axis_index(TQ)
    lanes = got_ref.shape[3]
    left = [got_ref[place ^ other].reshape(-1, lanes) for other in range(QUAD)]
    part = jnp.dot(
        jnp.concatenate(left, axis=1),
        jnp.concatenate([ref[0] for ref in weights], axis=0),
        preferred_element_type=f32,
    )
    out_ref[...] = part.astype(bf16).reshape(out_ref.shape)


def out_kernel(keep_ref, got_ref, own_ref, far_ref, out_ref):
    lanes = keep_ref.shape[2]
    left = [ref[...].reshape(-1, lanes) for ref in (keep_ref, got_ref)]
    part = jnp.dot(
        jnp.concatenate(left, axis=1),
        jnp.concatenate([own_ref[0], far_ref[0]], axis=0),
        preferred_element_type=f32,
    )
    out_ref[...] = part.astype(bf16).reshape(out_ref.shape)


def sum_parts(parts_ref):
    total = parts_ref[0].astype(f32)
    for t in range(1, parts_ref.shape[0]):
        total = total + parts_ref[t].astype(f32)
    return total


def join_kernel(steps, lens_ref, tokens_ref, parts_ref, gain_ref, out_ref):
    slots = parts_ref.shape[1]
    pick = compact_rows(
        lens_ref[...], slots, tokens_ref.shape[0], steps, lax.axis_index(TP) * slots
    )
    x = jnp.dot(pick, tokens_ref[...], preferred_element_type=f32)
    scaled = ((x + sum_parts(parts_ref)) * gain_ref[1:2]).astype(bf16)
    for t in range(out_ref.shape[0]):
        out_ref[t] = scaled


def final_kernel(parts_ref, resid_ref, out_ref):
    out_ref[...] = resid_ref[...] + sum_parts(parts_ref)


def body(
    tokens,
    lengths,
    norm_gain,
    w_recept,
    w_key,
    w_value,
    w_decay,
    w_rate,
    w_gate,
    w_out,
    decay_base,
    out_gain,
    states,
):
    own_seqs, steps, feats = tokens.shape
    th, xs = lax.axis_size(TH), lax.axis_size("x")
    tp = th * PAIR
    owners = xs * CORES
    own = own_seqs * steps
    rows = own * tp
    held = rows // owners
    seqs = states.shape[1]
    lanes = w_key.shape[2]
    width = 6 * lanes + LANES
    assert lanes == LANES and SLOTS * tp >= LIVE and seqs * steps == held

    lens_row = lengths.reshape(1, -1)
    mine = tokens.reshape(own, feats)
    weights = (w_recept, w_key, w_value, w_decay, w_rate, w_gate)

    def pick(block, shape):
        return pl.BlockSpec((1, *shape), lambda _: (block, *(0 for _ in shape)))

    def weight_specs(block):
        return [pick(block, (feats, lanes)) for _ in weights]

    pair = (pltpu.VMEM((xs, held, width), f32), pltpu.VMEM((xs, held, width), bf16))
    project_scratch = (
        pltpu.VMEM((owners, held, feats), bf16),
        pltpu.VMEM((owners, held, LANES), f32),
    )

    def exchange(keep, send):
        got = lax.ppermute(send, "c", swap)
        block = (held, width)
        own_part, *sends = call(
            add_kernel,
            (pltpu.VMEM(block, f32), *(pltpu.VMEM(block, bf16) for _ in range(1, xs))),
            [vmem(), vmem()],
        )(near(keep), near(got))
        far_first = sorted(enumerate(sends, 1), key=lambda pair: -min(pair[0], xs - pair[0]))
        return [own_part] + [
            lax.ppermute(send, "x", [(i, (i + shift) % xs) for i in range(xs)])
            for shift, send in far_first
        ]

    def mixed(block, parts, news):
        out_shape = (
            pltpu.VMEM((owners, held, lanes), bf16),
            jax.ShapeDtypeStruct(states.shape, f32),
        )
        extra = [] if news is None else [news]
        gated, news = call(
            functools.partial(mix_kernel, steps, block, xs),
            out_shape,
            [smem(), vmem(), vmem(), pick(block, states.shape[1:])]
            + [vmem()] * xs
            + [pl.BlockSpec(memory_space=pl.ANY)] * len(extra),
            (vmem(), pick(block, states.shape[1:])),
            input_output_aliases={4 + xs: 1} if extra else {},
        )(
            lengths,
            decay_base,
            out_gain,
            states,
            *(near(part) for part in parts),
            *extra,
        )
        gathered = lax.all_to_all(gated, DP, 0, 0, tiled=True)
        return gathered.reshape(rows, lanes), news

    swap = [(0, 1), (1, 0)]

    def gather(value):
        near_half = lax.all_to_all(value, TH, 0, 0, tiled=True)
        return near(near_half), near(lax.ppermute(near_half, "tl", swap))

    def from_place(value, other):
        return lax.ppermute(value, TQ, [(i, i ^ other) for i in range(QUAD)])

    w_far = from_place(w_out, 1)
    w_last = w_out[1:2]
    w_others = [from_place(w_last, other) for other in (2, 3)]
    everyone = near(lax.all_gather(mine, TP, axis=0, tiled=True))
    keep, send = call(
        first_kernel, pair, [vmem(), vmem(), *weight_specs(0)], scratch=project_scratch
    )(everyone, norm_gain, *(pltpu.with_memory_space_constraint(w, pltpu.HBM) for w in weights))
    gated, news = mixed(0, exchange(keep, send), None)
    gated, w_others = lax.optimization_barrier((gated, w_others))
    half = pltpu.VMEM((th, SLOTS, lanes), bf16)
    keep, send = call(
        functools.partial(pick_kernel, steps),
        (half, half),
        [vmem(), vmem()],
        scratch=(pltpu.VMEM((th, PAIR, SLOTS, lanes), bf16),),
    )(lens_row, near(gated))
    got = lax.ppermute(send, "tl", swap)
    partial = call(
        out_kernel,
        pltpu.VMEM((th, SLOTS, feats), bf16),
        [vmem(), vmem(), pick(0, (lanes, feats)), pick(0, (lanes, feats))],
    )(near(keep), near(got), w_out, w_far)
    partial = near(lax.all_to_all(partial, TH, 0, 0, tiled=True))
    scaled = call(
        functools.partial(join_kernel, steps),
        pltpu.VMEM((th, SLOTS, feats), bf16),
        [vmem(), vmem(), vmem(), vmem()],
    )(lens_row, everyone, partial, norm_gain)
    keep, send, resid = call(
        functools.partial(next_kernel, steps),
        (*pair, pltpu.VMEM((own, feats), f32)),
        [vmem(), vmem(), vmem(), vmem(), vmem(), *weight_specs(1)],
        scratch=(
            *project_scratch,
            pltpu.VMEM((tp, own, feats), f32),
            pltpu.VMEM((th, PAIR, SLOTS, feats), bf16),
        ),
    )(lens_row, *gather(scaled), mine, norm_gain, *weights)
    gated, news = mixed(1, exchange(keep, send), news)
    quads = tp // QUAD
    grouped = call(group_kernel, pltpu.VMEM((QUAD, quads, own, lanes), bf16), [vmem()])(near(gated))
    grouped = near(lax.all_to_all(grouped, TQ, 0, 0, tiled=True))
    partial = call(
        last_kernel,
        pltpu.VMEM((quads, own, feats), bf16),
        [vmem(), *(pick(1, (lanes, feats)) for _ in range(2)), vmem(), vmem()],
    )(grouped, w_out, w_far, *w_others)
    partial = near(lax.all_to_all(partial, "ta", 0, 0, tiled=True))
    stream = call(final_kernel, jax.ShapeDtypeStruct((own, feats), f32), [vmem(), vmem()])(
        partial, near(resid)
    )
    return stream.reshape(tokens.shape), news


def solution(mesh):
    split = Mesh(
        mesh.devices.reshape(
            mesh.shape["grp"],
            mesh.shape["tp"] // QUAD,
            QUAD // PAIR,
            PAIR,
            mesh.shape["dp"] // CORES,
            CORES,
        ),
        ("grp", *TP, "x", "c"),
    )
    return jax.shard_map(
        body,
        mesh=split,
        in_specs=(
            P(("grp", *TP), None, DP),
            P("grp"),
            P(None, DP),
            P(None, DP, TP),
            P(None, DP, TP),
            P(None, DP, TP),
            P(None, DP, TP),
            P(None, DP, TP),
            P(None, DP, TP),
            P(None, TP, DP),
            P(None, TP),
            P(None, TP),
            P(None, GRP_DP, None, TP),
        ),
        out_specs=(P(("grp", *TP), None, DP), P(None, GRP_DP, None, TP)),
        check_vma=False,
    )
```

```python
import functools

import jax
import jax.numpy as jnp
from jax import lax
from jax.experimental import pallas as pl
from jax.experimental.pallas import tpu as pltpu
from jax.sharding import Mesh
from jax.sharding import PartitionSpec as P

D = 4096
HEAD = 64
BLOCKS = 2
LANES = 128
CORES = 2
PAIR = 2
QUAD = 4
LIVE = 224
SLOTS = 16
LINES = 8
DP = ("x", "c")
TP = ("ta", "tm", "tl")
TH = ("ta", "tm")
TQ = ("tm", "tl")
GRP_DP = ("grp", "x", "c")

group_eps = 0.00064
norm_eps = 1e-06
key_eps = 1e-06
decay_scale = 0.606531


f32 = jnp.float32
bf16 = jnp.bfloat16


def iota(shape, dim):
    return lax.broadcasted_iota(jnp.int32, shape, dim)


def vmem():
    return pl.BlockSpec(memory_space=pltpu.VMEM)


def smem():
    return pl.BlockSpec(memory_space=pltpu.SMEM)


def near(value):
    return pltpu.with_memory_space_constraint(value, pltpu.VMEM)


def call(kernel, out_shape, in_specs, out_specs=None, scratch=(), **more):
    if out_specs is None:
        out_specs = tuple(vmem() for _ in out_shape) if isinstance(out_shape, tuple) else vmem()
    return pl.pallas_call(
        kernel,
        grid=(1,),
        out_shape=out_shape,
        in_specs=in_specs,
        out_specs=out_specs,
        scratch_shapes=list(scratch),
        compiler_params=pltpu.CompilerParams(vmem_limit_bytes=24 * 2**20),
        **more,
    )


def halves(value):
    high = value.astype(bf16)
    return high, (value - high.astype(f32)).astype(bf16)


def split_two(value):
    return jnp.concatenate(halves(value), axis=1)


def head_mask():
    rows, cols = iota((2 * LANES, LANES), 0), iota((2 * LANES, LANES), 1)
    return jnp.where((rows % LANES) // HEAD == cols // HEAD, 1.0, 0.0).astype(bf16)


def head_sum(value, mask):
    return jnp.dot(split_two(value), mask, preferred_element_type=f32)


def compact_rows(lens, slots, rows, steps, first):
    seqs = rows // steps
    seq_of = iota((seqs, rows), 1) // steps
    before = jnp.where(iota((seqs, rows), 0) < seq_of, 1.0, 0.0).astype(bf16)
    same = jnp.where(iota((seqs, rows), 0) == seq_of, 1.0, 0.0).astype(bf16)
    wide = jnp.broadcast_to(lens.astype(f32), (8, seqs)).astype(bf16)
    start = jnp.dot(wide, before, preferred_element_type=f32)[0:1]
    count = jnp.dot(wide, same, preferred_element_type=f32)[0:1]
    step = (iota((1, rows), 1) % steps).astype(f32)
    place = jnp.where(step < count, start + step, -1.0)
    slot = (iota((slots, rows), 0) + first).astype(f32)
    return jnp.where(slot == jnp.broadcast_to(place, (slots, rows)), 1.0, 0.0).astype(bf16)


def spread_rows(lens, rows, slots, steps):
    seqs = rows // steps
    wide = jnp.broadcast_to(lens.astype(f32), (rows, seqs))
    seq_of = iota((rows, seqs), 0) // steps
    start = jnp.sum(jnp.where(iota((rows, seqs), 1) < seq_of, wide, 0.0), axis=1, keepdims=True)
    count = jnp.sum(jnp.where(iota((rows, seqs), 1) == seq_of, wide, 0.0), axis=1, keepdims=True)
    step = (iota((rows, 1), 0) % steps).astype(f32)
    live = step < count
    place = jnp.where(live, start + step, -1.0)
    slot = iota((rows, slots), 1).astype(f32)
    return jnp.where(slot == jnp.broadcast_to(place, (rows, slots)), 1.0, 0.0).astype(bf16), live


def two_lanes(total):
    high = total.astype(bf16).astype(f32)
    return jnp.where(iota(total.shape, 1) < LANES // 2, high, total - high)


def project(weights, keep_ref, send_ref, scaled_scr, square_scr):
    owners = scaled_scr.shape[0]
    held = scaled_scr.shape[1]
    weight = jnp.concatenate([w[0] for w in weights], axis=1)
    core = lax.axis_index("c")
    diagonal = iota((held, LANES), 0) == iota((held, LANES), 1) % held
    for target, who in ((send_ref, 1 - core), (keep_ref, core)):
        left = jnp.concatenate([scaled_scr[CORES * x + who] for x in range(owners // CORES)], axis=0)
        part = jnp.dot(left, weight, preferred_element_type=f32)
        for x in range(owners // CORES):
            for i in range(len(weights)):
                piece = part[x * held : (x + 1) * held, i * LANES : (i + 1) * LANES]
                target[x, i * held : (i + 1) * held] = piece.astype(target.dtype)
            square = jnp.where(diagonal, square_scr[CORES * x + who], 0.0)
            square = jnp.broadcast_to(jnp.sum(square, axis=0, keepdims=True), (LINES, LANES))
            if target is send_ref:
                square = two_lanes(square)
            else:
                square = jnp.where(iota(square.shape, 1) < held, square, 0.0)
            target[x, len(weights) * held :] = square.astype(target.dtype)


def first_kernel(tokens_ref, gain_ref, *refs):
    weights, (keep_ref, send_ref, scaled_scr, square_scr) = refs[:6], refs[6:]
    x = tokens_ref[...].astype(f32)
    scaled_scr[...] = (x * gain_ref[0:1]).astype(bf16).reshape(scaled_scr.shape)
    squares = jnp.sum(x * x, axis=1, keepdims=True)
    square_scr[...] = jnp.broadcast_to(squares, (x.shape[0], LANES)).reshape(square_scr.shape)
    project(weights, keep_ref, send_ref, scaled_scr, square_scr)


def next_kernel(steps, lens_ref, near_ref, far_ref, tokens_ref, gain_ref, *refs):
    weights = refs[:6]
    keep_ref, send_ref, resid_ref, scaled_scr, square_scr, wide_scr, slot_scr = refs[6:]
    rows = scaled_scr.shape[0] * scaled_scr.shape[1]
    side = lax.axis_index("tl")
    for half_ref, place in ((near_ref, side), (far_ref, 1 - side)):
        slot_scr[:, place] = half_ref[...]
    slots = slot_scr[...].reshape(-1, slot_scr.shape[3])
    spread, live = spread_rows(lens_ref[...], rows, slots.shape[0], steps)
    wide = jnp.dot(spread, slots, preferred_element_type=f32)
    scaled_scr[...] = wide.astype(bf16).reshape(scaled_scr.shape)
    x = wide * (1.0 / gain_ref[1:2])
    squares = jnp.sum(x * x, axis=1, keepdims=True)
    own = resid_ref.shape[0]
    wide_scr[...] = x.reshape(wide_scr.shape)
    square_scr[...] = jnp.broadcast_to(jnp.where(live, 1.0, 0.0), (rows, LANES)).reshape(
        square_scr.shape
    )
    rank = lax.axis_index(TP)
    per = square_scr.shape[1] // own
    alive = square_scr[rank // per, pl.ds(pl.multiple_of((rank % per) * own, own), own), 0:1] > 0.5
    resid_ref[...] = jnp.where(alive, wide_scr[rank], tokens_ref[...].astype(f32))
    square_scr[...] = jnp.broadcast_to(squares, (rows, LANES)).reshape(square_scr.shape)
    project(weights, keep_ref, send_ref, scaled_scr, square_scr)


def add_kernel(keep_ref, got_ref, own_ref, *send_refs):
    rows = own_ref.shape[0] - LINES
    here, size = lax.axis_index("x"), keep_ref.shape[0]
    for shift, target in enumerate((own_ref, *send_refs)):
        x = (here + shift) % size
        total = keep_ref[x] + got_ref[x].astype(f32)
        square = total[rows:]
        square = square + pltpu.roll(square, LANES // 2, 1)
        target[:rows] = total[:rows].astype(target.dtype)
        target[rows:] = two_lanes(square).astype(target.dtype)


def mix_kernel(steps, block, size, lens_ref, base_ref, gain_ref, state_ref, *refs):
    parts = refs[:size]
    gated_ref, new_ref = refs[-2:]
    seqs = state_ref.shape[1]
    mask = head_mask()
    total = parts[0][...]
    for part in parts[1:]:
        total = total + part[...].astype(f32)
    held = seqs * steps
    square = total[6 * held : 6 * held + 1]
    square = square + pltpu.roll(square, LANES // 2, 1)
    square = jnp.broadcast_to(square, (held, LANES))
    square = jnp.where(iota((held, LANES), 0) == iota((held, LANES), 1), square, 0.0)
    inv_rms = lax.rsqrt(jnp.sum(square, axis=1, keepdims=True) * (1.0 / D) + norm_eps)
    recept, keys, values, decay_pre, rate_pre, gate_pre = (
        total[i * held : (i + 1) * held] * inv_rms for i in range(6)
    )
    first = lax.axis_index(DP) * seqs
    live = jnp.concatenate(
        [iota((steps, LANES), 0) < lens_ref[first + b] for b in range(seqs)], axis=0
    )
    fall = -decay_scale * jax.nn.sigmoid(decay_pre + base_ref[block : block + 1])
    fall = jnp.where(live, fall, 0.0)
    rate = jax.nn.sigmoid(rate_pre)
    unit = keys * lax.rsqrt(head_sum(keys * keys, mask) + key_eps)
    removal = jnp.where(live, unit * rate, 0.0)
    keys = jnp.where(live, keys, 0.0)
    rows = unit.shape[0]
    position = iota((rows, LANES), 0) % steps

    def row(value, s):
        value = value.reshape(seqs, steps, LANES)[:, s : s + 1]
        return jnp.broadcast_to(value, (seqs, steps, LANES)).reshape(rows, LANES)

    def cut(value, b):
        return value[b * steps : (b + 1) * steps]

    until, reach = fall, 1
    while reach < steps:
        until = until + jnp.where(position >= reach, pltpu.roll(until, reach, 0), 0.0)
        reach *= 2
    before = until - fall

    products = []
    for s in range(steps):
        until_s, keys_s, removal_s = row(until, s), row(keys, s), row(removal, s)
        seeing = jnp.where(position > s, unit * jnp.exp(before - until_s), 0.0)
        reading = jnp.where(position >= s, recept * jnp.exp(until - until_s), 0.0)
        products += [seeing * keys_s, seeing * removal_s, reading * keys_s, reading * removal_s]
    sums = head_sum(jnp.concatenate(products, axis=0), mask)
    pairs = [sums[i * rows : (i + 1) * rows] for i in range(4 * steps)]

    seeing, reading = unit * jnp.exp(before), recept * jnp.exp(until)
    lane = iota((HEAD, LANES), 1) < HEAD
    seen, read = [], []
    for b in range(seqs):
        left = jnp.concatenate([cut(seeing, b), cut(reading, b)], axis=0)
        high, low = halves(left)
        left = jnp.concatenate([high, low, high], axis=1)
        state = state_ref[0, b]
        high, low = halves(
            jnp.concatenate([jnp.where(lane, state, 0.0), jnp.where(lane, 0.0, state)], axis=0)
        )
        right = jnp.concatenate([high, high, low], axis=1)
        part = lax.dot_general(
            left, right, (((1,), (1,)), ((), ())), preferred_element_type=f32
        )
        seen.append(part[:steps])
        read.append(part[steps:])
    seen, read = jnp.concatenate(seen, axis=0), jnp.concatenate(read, axis=0)
    for s in range(steps):
        values_s = row(values, s)
        seen = seen + pairs[4 * s] * values_s
        read = read + pairs[4 * s + 2] * values_s
    for s in range(steps):
        seen_s = row(seen, s)
        seen = seen - pairs[4 * s + 1] * seen_s
        read = read - pairs[4 * s + 3] * seen_s

    last = row(until, steps - 1)
    onward = jnp.exp(last - until)
    keys, removal, last = keys * onward, removal * onward, jnp.exp(last)
    for b in range(seqs):
        high, low = halves(jnp.concatenate([cut(values, b), -cut(seen, b)], axis=0))
        left = jnp.concatenate([high, low, high], axis=0)
        high, low = halves(jnp.concatenate([cut(keys, b), cut(removal, b)], axis=0))
        right = jnp.concatenate([high, high, low], axis=0)
        part = lax.dot_general(
            left, right, (((0,), (0,)), ((), ())), preferred_element_type=f32
        )
        part = jnp.where(lane, part[:HEAD], part[HEAD:])
        new_ref[0, b] = state_ref[0, b] * last[b * steps : b * steps + 1] + part
    centered = read - head_sum(read, mask) * (1.0 / HEAD)
    spread = head_sum(centered * centered, mask) * (1.0 / HEAD)
    normed = centered * lax.rsqrt(spread + group_eps)
    gated = normed * gain_ref[block : block + 1] * jax.nn.sigmoid(gate_pre)
    gated = jnp.where(live, gated, 0.0).astype(bf16)
    for d in range(gated_ref.shape[0]):
        gated_ref[d] = gated


def halve(rows, keep_ref, send_ref, scr):
    side = lax.axis_index("tl")
    scr[...] = rows.reshape(scr.shape)
    keep_ref[...] = scr[:, side]
    send_ref[...] = scr[:, 1 - side]


def pick_kernel(steps, lens_ref, gated_ref, keep_ref, send_ref, scr):
    slots = scr.shape[0] * scr.shape[1] * scr.shape[2]
    pick = compact_rows(lens_ref[...], slots, gated_ref.shape[0], steps, 0)
    rows = jnp.dot(pick, gated_ref[...], preferred_element_type=f32).astype(bf16)
    halve(rows, keep_ref, send_ref, scr)


def group_kernel(gated_ref, out_ref):
    places, groups, own, _ = out_ref.shape
    for place in range(places):
        for group in range(groups):
            first = (group * places + place) * own
            out_ref[place, group] = gated_ref[first : first + own]


def last_kernel(got_ref, *refs):
    weights, out_ref = refs[:-1], refs[-1]
    place = lax.axis_index(TQ)
    lanes = got_ref.shape[3]
    left = [got_ref[place ^ other].reshape(-1, lanes) for other in range(QUAD)]
    part = jnp.dot(
        jnp.concatenate(left, axis=1),
        jnp.concatenate([ref[0] for ref in weights], axis=0),
        preferred_element_type=f32,
    )
    out_ref[...] = part.astype(bf16).reshape(out_ref.shape)


def out_kernel(keep_ref, got_ref, own_ref, far_ref, out_ref):
    lanes = keep_ref.shape[2]
    left = [ref[...].reshape(-1, lanes) for ref in (keep_ref, got_ref)]
    part = jnp.dot(
        jnp.concatenate(left, axis=1),
        jnp.concatenate([own_ref[0], far_ref[0]], axis=0),
        preferred_element_type=f32,
    )
    out_ref[...] = part.astype(bf16).reshape(out_ref.shape)


def sum_parts(parts_ref):
    total = parts_ref[0].astype(f32)
    for t in range(1, parts_ref.shape[0]):
        total = total + parts_ref[t].astype(f32)
    return total


def join_kernel(steps, lens_ref, tokens_ref, parts_ref, gain_ref, out_ref):
    slots = parts_ref.shape[1]
    pick = compact_rows(
        lens_ref[...], slots, tokens_ref.shape[0], steps, lax.axis_index(TP) * slots
    )
    x = jnp.dot(pick, tokens_ref[...], preferred_element_type=f32)
    scaled = ((x + sum_parts(parts_ref)) * gain_ref[1:2]).astype(bf16)
    for t in range(out_ref.shape[0]):
        out_ref[t] = scaled


def final_kernel(parts_ref, resid_ref, out_ref):
    out_ref[...] = resid_ref[...] + sum_parts(parts_ref)


def body(
    tokens,
    lengths,
    norm_gain,
    w_recept,
    w_key,
    w_value,
    w_decay,
    w_rate,
    w_gate,
    w_out,
    decay_base,
    out_gain,
    states,
):
    own_seqs, steps, feats = tokens.shape
    th, xs = lax.axis_size(TH), lax.axis_size("x")
    tp = th * PAIR
    owners = xs * CORES
    own = own_seqs * steps
    rows = own * tp
    held = rows // owners
    seqs = states.shape[1]
    lanes = w_key.shape[2]
    lines = 6 * held + LINES
    assert lanes == LANES and SLOTS * tp >= LIVE and seqs * steps == held
    assert 2 * held == LANES

    lens_row = lengths.reshape(1, -1)
    mine = tokens.reshape(own, feats)
    weights = (w_recept, w_key, w_value, w_decay, w_rate, w_gate)

    def pick(block, shape):
        return pl.BlockSpec((1, *shape), lambda _: (block, *(0 for _ in shape)))

    def weight_specs(block):
        return [pick(block, (feats, lanes)) for _ in weights]

    pair = (pltpu.VMEM((xs, lines, lanes), f32), pltpu.VMEM((xs, lines, lanes), bf16))
    project_scratch = (
        pltpu.VMEM((owners, held, feats), bf16),
        pltpu.VMEM((owners, held, LANES), f32),
    )

    def exchange(keep, send):
        got = lax.ppermute(send, "c", swap)
        block = (lines, lanes)
        own_part, *sends = call(
            add_kernel,
            (pltpu.VMEM(block, f32), *(pltpu.VMEM(block, bf16) for _ in range(1, xs))),
            [vmem(), vmem()],
        )(near(keep), near(got))
        far_first = sorted(enumerate(sends, 1), key=lambda pair: -min(pair[0], xs - pair[0]))
        return [own_part] + [
            lax.ppermute(send, "x", [(i, (i + shift) % xs) for i in range(xs)])
            for shift, send in far_first
        ]

    def mixed(block, parts, news):
        out_shape = (
            pltpu.VMEM((owners, held, lanes), bf16),
            jax.ShapeDtypeStruct(states.shape, f32),
        )
        extra = [] if news is None else [news]
        gated, news = call(
            functools.partial(mix_kernel, steps, block, xs),
            out_shape,
            [smem(), vmem(), vmem(), pick(block, states.shape[1:])]
            + [vmem()] * xs
            + [pl.BlockSpec(memory_space=pl.ANY)] * len(extra),
            (vmem(), pick(block, states.shape[1:])),
            input_output_aliases={4 + xs: 1} if extra else {},
        )(
            lengths,
            decay_base,
            out_gain,
            states,
            *(near(part) for part in parts),
            *extra,
        )
        gathered = lax.all_to_all(gated, DP, 0, 0, tiled=True)
        return gathered.reshape(rows, lanes), news

    swap = [(0, 1), (1, 0)]

    def gather(value):
        near_half = lax.all_to_all(value, TH, 0, 0, tiled=True)
        return near(near_half), near(lax.ppermute(near_half, "tl", swap))

    def from_place(value, other):
        return lax.ppermute(value, TQ, [(i, i ^ other) for i in range(QUAD)])

    w_far = from_place(w_out, 1)
    w_last = w_out[1:2]
    w_others = [from_place(w_last, other) for other in (2, 3)]
    everyone = near(lax.all_gather(mine, TP, axis=0, tiled=True))
    keep, send = call(
        first_kernel, pair, [vmem(), vmem(), *weight_specs(0)], scratch=project_scratch
    )(everyone, norm_gain, *(pltpu.with_memory_space_constraint(w, pltpu.HBM) for w in weights))
    gated, news = mixed(0, exchange(keep, send), None)
    gated, w_others = lax.optimization_barrier((gated, w_others))
    half = pltpu.VMEM((th, SLOTS, lanes), bf16)
    keep, send = call(
        functools.partial(pick_kernel, steps),
        (half, half),
        [vmem(), vmem()],
        scratch=(pltpu.VMEM((th, PAIR, SLOTS, lanes), bf16),),
    )(lens_row, near(gated))
    got = lax.ppermute(send, "tl", swap)
    partial = call(
        out_kernel,
        pltpu.VMEM((th, SLOTS, feats), bf16),
        [vmem(), vmem(), pick(0, (lanes, feats)), pick(0, (lanes, feats))],
    )(near(keep), near(got), w_out, w_far)
    partial = near(lax.all_to_all(partial, TH, 0, 0, tiled=True))
    scaled = call(
        functools.partial(join_kernel, steps),
        pltpu.VMEM((th, SLOTS, feats), bf16),
        [vmem(), vmem(), vmem(), vmem()],
    )(lens_row, everyone, partial, norm_gain)
    keep, send, resid = call(
        functools.partial(next_kernel, steps),
        (*pair, pltpu.VMEM((own, feats), f32)),
        [vmem(), vmem(), vmem(), vmem(), vmem(), *weight_specs(1)],
        scratch=(
            *project_scratch,
            pltpu.VMEM((tp, own, feats), f32),
            pltpu.VMEM((th, PAIR, SLOTS, feats), bf16),
        ),
    )(lens_row, *gather(scaled), mine, norm_gain, *weights)
    gated, news = mixed(1, exchange(keep, send), news)
    quads = tp // QUAD
    grouped = call(group_kernel, pltpu.VMEM((QUAD, quads, own, lanes), bf16), [vmem()])(near(gated))
    grouped = near(lax.all_to_all(grouped, TQ, 0, 0, tiled=True))
    partial = call(
        last_kernel,
        pltpu.VMEM((quads, own, feats), bf16),
        [vmem(), *(pick(1, (lanes, feats)) for _ in range(2)), vmem(), vmem()],
    )(grouped, w_out, w_far, *w_others)
    partial = near(lax.all_to_all(partial, "ta", 0, 0, tiled=True))
    stream = call(final_kernel, jax.ShapeDtypeStruct((own, feats), f32), [vmem(), vmem()])(
        partial, near(resid)
    )
    return stream.reshape(tokens.shape), news


def solution(mesh):
    split = Mesh(
        mesh.devices.reshape(
            mesh.shape["grp"],
            mesh.shape["tp"] // QUAD,
            QUAD // PAIR,
            PAIR,
            mesh.shape["dp"] // CORES,
            CORES,
        ),
        ("grp", *TP, "x", "c"),
    )
    return jax.shard_map(
        body,
        mesh=split,
        in_specs=(
            P(("grp", *TP), None, DP),
            P("grp"),
            P(None, DP),
            P(None, DP, TP),
            P(None, DP, TP),
            P(None, DP, TP),
            P(None, DP, TP),
            P(None, DP, TP),
            P(None, DP, TP),
            P(None, TP, DP),
            P(None, TP),
            P(None, TP),
            P(None, GRP_DP, None, TP),
        ),
        out_specs=(P(("grp", *TP), None, DP), P(None, GRP_DP, None, TP)),
        check_vma=False,
    )
```

```python
import functools

import jax
import jax.numpy as jnp
from jax import lax
from jax.experimental import pallas as pl
from jax.experimental.pallas import tpu as pltpu
from jax.sharding import Mesh
from jax.sharding import PartitionSpec as P

D = 4096
HEAD = 64
BLOCKS = 2
LANES = 128
CORES = 2
PAIR = 2
QUAD = 4
LIVE = 224
SLOTS = 16
LINES = 8
DP = ("x", "c")
TP = ("ta", "tm", "tl")
TH = ("ta", "tm")
TQ = ("tm", "tl")
GRP_DP = ("grp", "x", "c")

group_eps = 0.00064
norm_eps = 1e-06
key_eps = 1e-06
decay_scale = 0.606531


f32 = jnp.float32
bf16 = jnp.bfloat16


def iota(shape, dim):
    return lax.broadcasted_iota(jnp.int32, shape, dim)


def vmem():
    return pl.BlockSpec(memory_space=pltpu.VMEM)


def smem():
    return pl.BlockSpec(memory_space=pltpu.SMEM)


def near(value):
    return pltpu.with_memory_space_constraint(value, pltpu.VMEM)


def call(kernel, out_shape, in_specs, out_specs=None, scratch=(), **more):
    if out_specs is None:
        out_specs = tuple(vmem() for _ in out_shape) if isinstance(out_shape, tuple) else vmem()
    return pl.pallas_call(
        kernel,
        grid=(1,),
        out_shape=out_shape,
        in_specs=in_specs,
        out_specs=out_specs,
        scratch_shapes=list(scratch),
        compiler_params=pltpu.CompilerParams(vmem_limit_bytes=24 * 2**20),
        **more,
    )


def halves(value):
    high = value.astype(bf16)
    return high, (value - high.astype(f32)).astype(bf16)


def split_two(value):
    return jnp.concatenate(halves(value), axis=1)


def head_mask():
    rows, cols = iota((2 * LANES, LANES), 0), iota((2 * LANES, LANES), 1)
    return jnp.where((rows % LANES) // HEAD == cols // HEAD, 1.0, 0.0).astype(bf16)


def head_sum(value, mask):
    return jnp.dot(split_two(value), mask, preferred_element_type=f32)


def compact_rows(lens, slots, rows, steps, first):
    seqs = rows // steps
    seq_of = iota((seqs, rows), 1) // steps
    before = jnp.where(iota((seqs, rows), 0) < seq_of, 1.0, 0.0).astype(bf16)
    same = jnp.where(iota((seqs, rows), 0) == seq_of, 1.0, 0.0).astype(bf16)
    wide = jnp.broadcast_to(lens.astype(f32), (8, seqs)).astype(bf16)
    start = jnp.dot(wide, before, preferred_element_type=f32)[0:1]
    count = jnp.dot(wide, same, preferred_element_type=f32)[0:1]
    step = (iota((1, rows), 1) % steps).astype(f32)
    place = jnp.where(step < count, start + step, -1.0)
    slot = (iota((slots, rows), 0) + first).astype(f32)
    return jnp.where(slot == jnp.broadcast_to(place, (slots, rows)), 1.0, 0.0).astype(bf16)


def spread_rows(lens, rows, slots, steps):
    seqs = rows // steps
    wide = jnp.broadcast_to(lens.astype(f32), (rows, seqs))
    seq_of = iota((rows, seqs), 0) // steps
    start = jnp.sum(jnp.where(iota((rows, seqs), 1) < seq_of, wide, 0.0), axis=1, keepdims=True)
    count = jnp.sum(jnp.where(iota((rows, seqs), 1) == seq_of, wide, 0.0), axis=1, keepdims=True)
    step = (iota((rows, 1), 0) % steps).astype(f32)
    live = step < count
    place = jnp.where(live, start + step, -1.0)
    slot = iota((rows, slots), 1).astype(f32)
    return jnp.where(slot == jnp.broadcast_to(place, (rows, slots)), 1.0, 0.0).astype(bf16), live


def two_lanes(total):
    high = total.astype(bf16).astype(f32)
    return jnp.where(iota(total.shape, 1) < LANES // 2, high, total - high)


def project(weights, keep_ref, send_ref, scaled_scr, square_scr):
    owners = scaled_scr.shape[0]
    held = scaled_scr.shape[1]
    weight = jnp.concatenate([w[0] for w in weights], axis=1)
    core = lax.axis_index("c")
    diagonal = iota((held, LANES), 0) == iota((held, LANES), 1) % held
    for target, who in ((send_ref, 1 - core), (keep_ref, core)):
        left = jnp.concatenate([scaled_scr[CORES * x + who] for x in range(owners // CORES)], axis=0)
        part = jnp.dot(left, weight, preferred_element_type=f32)
        for x in range(owners // CORES):
            for i in range(len(weights)):
                piece = part[x * held : (x + 1) * held, i * LANES : (i + 1) * LANES]
                target[x, i * held : (i + 1) * held] = piece.astype(target.dtype)
            square = jnp.where(diagonal, square_scr[CORES * x + who], 0.0)
            square = jnp.broadcast_to(jnp.sum(square, axis=0, keepdims=True), (LINES, LANES))
            if target is send_ref:
                square = two_lanes(square)
            else:
                square = jnp.where(iota(square.shape, 1) < held, square, 0.0)
            target[x, len(weights) * held :] = square.astype(target.dtype)


def first_kernel(tokens_ref, gain_ref, *refs):
    weights, (keep_ref, send_ref, scaled_scr, square_scr) = refs[:6], refs[6:]
    x = tokens_ref[...].astype(f32)
    scaled_scr[...] = (x * gain_ref[0:1]).astype(bf16).reshape(scaled_scr.shape)
    squares = jnp.sum(x * x, axis=1, keepdims=True)
    square_scr[...] = jnp.broadcast_to(squares, (x.shape[0], LANES)).reshape(square_scr.shape)
    project(weights, keep_ref, send_ref, scaled_scr, square_scr)


def next_kernel(steps, lens_ref, near_ref, far_ref, tokens_ref, gain_ref, *refs):
    weights = refs[:6]
    keep_ref, send_ref, resid_ref, scaled_scr, square_scr, wide_scr, slot_scr = refs[6:]
    rows = scaled_scr.shape[0] * scaled_scr.shape[1]
    side = lax.axis_index("tl")
    for half_ref, place in ((near_ref, side), (far_ref, 1 - side)):
        slot_scr[:, place] = half_ref[...]
    slots = slot_scr[...].reshape(-1, slot_scr.shape[3])
    spread, live = spread_rows(lens_ref[...], rows, slots.shape[0], steps)
    wide = jnp.dot(spread, slots, preferred_element_type=f32)
    scaled_scr[...] = wide.astype(bf16).reshape(scaled_scr.shape)
    x = wide * (1.0 / gain_ref[1:2])
    squares = jnp.sum(x * x, axis=1, keepdims=True)
    own = resid_ref.shape[0]
    wide_scr[...] = x.reshape(wide_scr.shape)
    square_scr[...] = jnp.broadcast_to(jnp.where(live, 1.0, 0.0), (rows, LANES)).reshape(
        square_scr.shape
    )
    rank = lax.axis_index(TP)
    per = square_scr.shape[1] // own
    alive = square_scr[rank // per, pl.ds(pl.multiple_of((rank % per) * own, own), own), 0:1] > 0.5
    resid_ref[...] = jnp.where(alive, wide_scr[rank], tokens_ref[...].astype(f32))
    square_scr[...] = jnp.broadcast_to(squares, (rows, LANES)).reshape(square_scr.shape)
    project(weights, keep_ref, send_ref, scaled_scr, square_scr)


def add_kernel(keep_ref, got_ref, own_ref, *send_refs):
    rows = own_ref.shape[0] - LINES
    here, size = lax.axis_index("x"), keep_ref.shape[0]
    for shift, target in enumerate((own_ref, *send_refs)):
        x = (here + shift) % size
        total = keep_ref[x] + got_ref[x].astype(f32)
        square = total[rows:]
        square = square + pltpu.roll(square, LANES // 2, 1)
        target[:rows] = total[:rows].astype(target.dtype)
        target[rows:] = two_lanes(square).astype(target.dtype)


def mix_kernel(steps, block, size, lens_ref, base_ref, gain_ref, state_ref, *refs):
    parts = refs[:size]
    gated_ref, new_ref = refs[-2:]
    seqs = state_ref.shape[1]
    mask = head_mask()
    total = parts[0][...]
    for part in parts[1:]:
        total = total + part[...].astype(f32)
    held = seqs * steps
    square = total[6 * held : 6 * held + 1]
    square = square + pltpu.roll(square, LANES // 2, 1)
    square = jnp.broadcast_to(square, (held, LANES))
    square = jnp.where(iota((held, LANES), 0) == iota((held, LANES), 1), square, 0.0)
    inv_rms = lax.rsqrt(jnp.sum(square, axis=1, keepdims=True) * (1.0 / D) + norm_eps)
    recept, keys, values, decay_pre, rate_pre, gate_pre = (
        total[i * held : (i + 1) * held] * inv_rms for i in range(6)
    )
    first = lax.axis_index(DP) * seqs
    live = jnp.concatenate(
        [iota((steps, LANES), 0) < lens_ref[first + b] for b in range(seqs)], axis=0
    )
    fall = -decay_scale * jax.nn.sigmoid(decay_pre + base_ref[block : block + 1])
    fall = jnp.where(live, fall, 0.0)
    rate = jax.nn.sigmoid(rate_pre)
    unit = keys * lax.rsqrt(head_sum(keys * keys, mask) + key_eps)
    removal = jnp.where(live, unit * rate, 0.0)
    keys = jnp.where(live, keys, 0.0)
    rows = unit.shape[0]
    position = iota((rows, LANES), 0) % steps

    def row(value, s):
        value = value.reshape(seqs, steps, LANES)[:, s : s + 1]
        return jnp.broadcast_to(value, (seqs, steps, LANES)).reshape(rows, LANES)

    def cut(value, b):
        return value[b * steps : (b + 1) * steps]

    until, reach = fall, 1
    while reach < steps:
        until = until + jnp.where(position >= reach, pltpu.roll(until, reach, 0), 0.0)
        reach *= 2
    before = until - fall

    products = []
    for s in range(steps):
        until_s, keys_s, removal_s = row(until, s), row(keys, s), row(removal, s)
        seeing = jnp.where(position > s, unit * jnp.exp(before - until_s), 0.0)
        reading = jnp.where(position >= s, recept * jnp.exp(until - until_s), 0.0)
        products += [seeing * keys_s, seeing * removal_s, reading * keys_s, reading * removal_s]
    sums = head_sum(jnp.concatenate(products, axis=0), mask)
    pairs = [sums[i * rows : (i + 1) * rows] for i in range(4 * steps)]

    seeing, reading = unit * jnp.exp(before), recept * jnp.exp(until)
    lane = iota((HEAD, LANES), 1) < HEAD
    seen, read = [], []
    for b in range(seqs):
        left = jnp.concatenate([cut(seeing, b), cut(reading, b)], axis=0)
        high, low = halves(left)
        left = jnp.concatenate([high, low, high], axis=1)
        state = state_ref[0, b]
        high, low = halves(
            jnp.concatenate([jnp.where(lane, state, 0.0), jnp.where(lane, 0.0, state)], axis=0)
        )
        right = jnp.concatenate([high, high, low], axis=1)
        part = lax.dot_general(
            left, right, (((1,), (1,)), ((), ())), preferred_element_type=f32
        )
        seen.append(part[:steps])
        read.append(part[steps:])
    seen, read = jnp.concatenate(seen, axis=0), jnp.concatenate(read, axis=0)
    for s in range(steps):
        values_s = row(values, s)
        seen = seen + pairs[4 * s] * values_s
        read = read + pairs[4 * s + 2] * values_s
    for s in range(steps):
        seen_s = row(seen, s)
        seen = seen - pairs[4 * s + 1] * seen_s
        read = read - pairs[4 * s + 3] * seen_s

    last = row(until, steps - 1)
    onward = jnp.exp(last - until)
    keys, removal, last = keys * onward, removal * onward, jnp.exp(last)
    for b in range(seqs):
        high, low = halves(jnp.concatenate([cut(values, b), -cut(seen, b)], axis=0))
        left = jnp.concatenate([high, low, high], axis=0)
        high, low = halves(jnp.concatenate([cut(keys, b), cut(removal, b)], axis=0))
        right = jnp.concatenate([high, high, low], axis=0)
        part = lax.dot_general(
            left, right, (((0,), (0,)), ((), ())), preferred_element_type=f32
        )
        part = jnp.where(lane, part[:HEAD], part[HEAD:])
        new_ref[0, b] = state_ref[0, b] * last[b * steps : b * steps + 1] + part
    centered = read - head_sum(read, mask) * (1.0 / HEAD)
    spread = head_sum(centered * centered, mask) * (1.0 / HEAD)
    normed = centered * lax.rsqrt(spread + group_eps)
    gated = normed * gain_ref[block : block + 1] * jax.nn.sigmoid(gate_pre)
    gated = jnp.where(live, gated, 0.0).astype(bf16)
    for d in range(gated_ref.shape[0]):
        gated_ref[d] = gated


def halve(rows, keep_ref, send_ref, scr):
    side = lax.axis_index("tl")
    scr[...] = rows.reshape(scr.shape)
    keep_ref[...] = scr[:, side]
    send_ref[...] = scr[:, 1 - side]


def pick_kernel(steps, lens_ref, gated_ref, keep_ref, send_ref, scr):
    slots = scr.shape[0] * scr.shape[1] * scr.shape[2]
    pick = compact_rows(lens_ref[...], slots, gated_ref.shape[0], steps, 0)
    rows = jnp.dot(pick, gated_ref[...], preferred_element_type=f32).astype(bf16)
    halve(rows, keep_ref, send_ref, scr)


def group_kernel(gated_ref, out_ref):
    places, groups, own, _ = out_ref.shape
    for place in range(places):
        for group in range(groups):
            first = (group * places + place) * own
            out_ref[place, group] = gated_ref[first : first + own]


def last_kernel(got_ref, *refs):
    weights, out_ref = refs[:-1], refs[-1]
    place = lax.axis_index(TQ)
    lanes = got_ref.shape[3]
    left = [got_ref[place ^ other].reshape(-1, lanes) for other in range(QUAD)]
    part = jnp.dot(
        jnp.concatenate(left, axis=1),
        jnp.concatenate([ref[0] for ref in weights], axis=0),
        preferred_element_type=f32,
    )
    out_ref[...] = part.astype(bf16).reshape(out_ref.shape)


def out_kernel(keep_ref, got_ref, own_ref, far_ref, out_ref):
    lanes = keep_ref.shape[2]
    left = [ref[...].reshape(-1, lanes) for ref in (keep_ref, got_ref)]
    part = jnp.dot(
        jnp.concatenate(left, axis=1),
        jnp.concatenate([own_ref[0], far_ref[0]], axis=0),
        preferred_element_type=f32,
    )
    out_ref[...] = part.astype(bf16).reshape(out_ref.shape)


def sum_parts(parts_ref):
    total = parts_ref[0].astype(f32)
    for t in range(1, parts_ref.shape[0]):
        total = total + parts_ref[t].astype(f32)
    return total


def join_kernel(steps, lens_ref, tokens_ref, parts_ref, gain_ref, out_ref):
    slots = parts_ref.shape[1]
    pick = compact_rows(
        lens_ref[...], slots, tokens_ref.shape[0], steps, lax.axis_index(TP) * slots
    )
    x = jnp.dot(pick, tokens_ref[...], preferred_element_type=f32)
    scaled = ((x + sum_parts(parts_ref)) * gain_ref[1:2]).astype(bf16)
    for t in range(out_ref.shape[0]):
        out_ref[t] = scaled


def final_kernel(parts_ref, resid_ref, out_ref):
    out_ref[...] = resid_ref[...] + sum_parts(parts_ref)


def body(
    tokens,
    lengths,
    norm_gain,
    w_recept,
    w_key,
    w_value,
    w_decay,
    w_rate,
    w_gate,
    w_out,
    decay_base,
    out_gain,
    states,
):
    own_seqs, steps, feats = tokens.shape
    th, xs = lax.axis_size(TH), lax.axis_size("x")
    tp = th * PAIR
    owners = xs * CORES
    own = own_seqs * steps
    rows = own * tp
    held = rows // owners
    seqs = states.shape[1]
    lanes = w_key.shape[2]
    lines = 6 * held + LINES
    assert lanes == LANES and SLOTS * tp >= LIVE and seqs * steps == held
    assert 2 * held == LANES

    lens_row = lengths.reshape(1, -1)
    mine = tokens.reshape(own, feats)
    weights = (w_recept, w_key, w_value, w_decay, w_rate, w_gate)

    def pick(block, shape):
        return pl.BlockSpec((1, *shape), lambda _: (block, *(0 for _ in shape)))

    def weight_specs(block):
        return [pick(block, (feats, lanes)) for _ in weights]

    pair = (pltpu.VMEM((xs, lines, lanes), f32), pltpu.VMEM((xs, lines, lanes), bf16))
    project_scratch = (
        pltpu.VMEM((owners, held, feats), bf16),
        pltpu.VMEM((owners, held, LANES), f32),
    )

    def exchange(keep, send):
        got = lax.ppermute(send, "c", swap)
        block = (lines, lanes)
        own_part, *sends = call(
            add_kernel,
            (pltpu.VMEM(block, f32), *(pltpu.VMEM(block, bf16) for _ in range(1, xs))),
            [vmem(), vmem()],
        )(near(keep), near(got))
        far_first = sorted(enumerate(sends, 1), key=lambda pair: -min(pair[0], xs - pair[0]))
        return [own_part] + [
            lax.ppermute(send, "x", [(i, (i + shift) % xs) for i in range(xs)])
            for shift, send in far_first
        ]

    def mixed(block, parts, news):
        out_shape = (
            pltpu.VMEM((owners, held, lanes), bf16),
            jax.ShapeDtypeStruct(states.shape, f32),
        )
        extra = [] if news is None else [news]
        gated, news = call(
            functools.partial(mix_kernel, steps, block, xs),
            out_shape,
            [smem(), vmem(), vmem(), pick(block, states.shape[1:])]
            + [vmem()] * xs
            + [pl.BlockSpec(memory_space=pl.ANY)] * len(extra),
            (vmem(), pick(block, states.shape[1:])),
            input_output_aliases={4 + xs: 1} if extra else {},
        )(
            lengths,
            decay_base,
            out_gain,
            states,
            *(near(part) for part in parts),
            *extra,
        )
        gathered = lax.all_to_all(gated, DP, 0, 0, tiled=True)
        return gathered.reshape(rows, lanes), news

    swap = [(0, 1), (1, 0)]

    def gather(value):
        near_half = lax.all_to_all(value, TH, 0, 0, tiled=True)
        return near(near_half), near(lax.ppermute(near_half, "tl", swap))

    def from_place(value, other):
        return lax.ppermute(value, TQ, [(i, i ^ other) for i in range(QUAD)])

    w_far = from_place(w_out, 1)
    w_last = w_out[1:2]
    w_others = [from_place(w_last, other) for other in (2, 3)]
    everyone = near(lax.all_gather(mine, TP, axis=0, tiled=True))
    keep, send = call(
        first_kernel, pair, [vmem(), vmem(), *weight_specs(0)], scratch=project_scratch
    )(
        everyone,
        norm_gain,
        *weights[:2],
        *(pltpu.with_memory_space_constraint(w, pltpu.HBM) for w in weights[2:]),
    )
    gated, news = mixed(0, exchange(keep, send), None)
    gated, w_others = lax.optimization_barrier((gated, w_others))
    half = pltpu.VMEM((th, SLOTS, lanes), bf16)
    keep, send = call(
        functools.partial(pick_kernel, steps),
        (half, half),
        [vmem(), vmem()],
        scratch=(pltpu.VMEM((th, PAIR, SLOTS, lanes), bf16),),
    )(lens_row, near(gated))
    got = lax.ppermute(send, "tl", swap)
    partial = call(
        out_kernel,
        pltpu.VMEM((th, SLOTS, feats), bf16),
        [vmem(), vmem(), pick(0, (lanes, feats)), pick(0, (lanes, feats))],
    )(near(keep), near(got), w_out, w_far)
    partial = near(lax.all_to_all(partial, TH, 0, 0, tiled=True))
    scaled = call(
        functools.partial(join_kernel, steps),
        pltpu.VMEM((th, SLOTS, feats), bf16),
        [vmem(), vmem(), vmem(), vmem()],
    )(lens_row, everyone, partial, norm_gain)
    keep, send, resid = call(
        functools.partial(next_kernel, steps),
        (*pair, pltpu.VMEM((own, feats), f32)),
        [vmem(), vmem(), vmem(), vmem(), vmem(), *weight_specs(1)],
        scratch=(
            *project_scratch,
            pltpu.VMEM((tp, own, feats), f32),
            pltpu.VMEM((th, PAIR, SLOTS, feats), bf16),
        ),
    )(lens_row, *gather(scaled), mine, norm_gain, *weights)
    gated, news = mixed(1, exchange(keep, send), news)
    quads = tp // QUAD
    grouped = call(group_kernel, pltpu.VMEM((QUAD, quads, own, lanes), bf16), [vmem()])(near(gated))
    grouped = near(lax.all_to_all(grouped, TQ, 0, 0, tiled=True))
    partial = call(
        last_kernel,
        pltpu.VMEM((quads, own, feats), bf16),
        [vmem(), *(pick(1, (lanes, feats)) for _ in range(2)), vmem(), vmem()],
    )(grouped, w_out, w_far, *w_others)
    partial = near(lax.all_to_all(partial, "ta", 0, 0, tiled=True))
    stream = call(final_kernel, jax.ShapeDtypeStruct((own, feats), f32), [vmem(), vmem()])(
        partial, near(resid)
    )
    return stream.reshape(tokens.shape), news


def solution(mesh):
    split = Mesh(
        mesh.devices.reshape(
            mesh.shape["grp"],
            mesh.shape["tp"] // QUAD,
            QUAD // PAIR,
            PAIR,
            mesh.shape["dp"] // CORES,
            CORES,
        ),
        ("grp", *TP, "x", "c"),
    )
    return jax.shard_map(
        body,
        mesh=split,
        in_specs=(
            P(("grp", *TP), None, DP),
            P("grp"),
            P(None, DP),
            P(None, DP, TP),
            P(None, DP, TP),
            P(None, DP, TP),
            P(None, DP, TP),
            P(None, DP, TP),
            P(None, DP, TP),
            P(None, TP, DP),
            P(None, TP),
            P(None, TP),
            P(None, GRP_DP, None, TP),
        ),
        out_specs=(P(("grp", *TP), None, DP), P(None, GRP_DP, None, TP)),
        check_vma=False,
    )
```
